512 devices in a mesh: ep: 16 (over y, x), tp: 32 (over z, core).
Axes of the slice: x: 4, y: 4, z: 16, core: 2. Of those that a mesh axis runs over, the one named last changes fastest.
Arguments:
- features: bfloat16 [256, 1024], P('ep', 'tp'), may hold values from -6 to 6
- key_table: bfloat16 [262144, 1024], P('ep', 'tp'), may hold values from -0.1875 to 0.1875
- value_table: bfloat16 [262144, 1024], P('ep', 'tp'), may hold values from -6 to 6
- chosen: int32 [256, 4, 16], P('ep'), may hold values from 0 to 262143
- scores: float32 [256, 4, 16], P('ep'), may hold values from -8 to 8
Outputs:
- mixed: bfloat16 [256, 1024], P('ep', 'tp')
The draws below stay inside these ranges and needn't reach their ends.
Inputs may be any that keep to these rules, and one draw needn't show every extreme that they name: Every chosen row is a row of the tables, 0 to 262143; rows may repeat, and a few rows are far more popular than the rest.
All inputs are finite; a program needn't handle non-finite values.
Results may differ from the reference program's by a relative error of at most 0.0065.
Values may be sent and summed in bfloat16 or wider, within the bound.
A program may use at most 64 MiB of HBM per device.

```python
import math
import jax
import jax.numpy as jnp
import numpy as np
from jax import lax

D = 1024
HEADS = 4
TOPK = 16
TOK_DEV = 16
TOKENS = 256
EXPERTS = 262144


def plant(result, rng, low, largest):
    index_at = [jax.random.randint(jax.random.fold_in(rng, axis), (), 0, length) for axis, length in enumerate(result.shape)]
    main_axis = result.shape.index(max(result.shape))
    neighbour = index_at[:main_axis] + [(index_at[main_axis] + 1) % result.shape[main_axis]] + index_at[main_axis + 1:]
    return result.at[tuple(index_at)].set(low).at[tuple(neighbour)].set(largest)


def shard_levels(key, extent, cuts, least, top_value):
    def one(dim, shards_of):
        steps = jax.random.uniform(jax.random.fold_in(jax.random.fold_in(key, 6), dim), (shards_of,), jnp.float32, least / len(cuts), top_value / len(cuts))
        return jnp.repeat(jnp.exp(steps), extent[dim] // shards_of).reshape((-1,) + (1,) * (len(extent) - dim - 1))

    level = one(*cuts[0])
    for cut in cuts[1:]:
        level = level * one(*cut)
    return level


def ranked_wide(own_key, shape, number_of, lean):
    loads = [min(1 << octave, number_of + 1 - (1 << octave)) * (1 << 20) // math.isqrt((1 << octave) ** lean) + 1 for octave in range((number_of + 1).bit_length()) if 1 << octave <= number_of]
    scale = 1 + sum(loads) // (1 << 30)
    listing = np.cumsum(np.array([max(1, weight // scale) for weight in loads]))
    lot = jax.random.randint(jax.random.fold_in(own_key, 1), shape, 0, int(listing[len(loads) - 1]))
    start = jnp.left_shift(1, jnp.searchsorted(jnp.asarray(listing, jnp.int32), lot, side="right").astype(jnp.int32))
    grade = start - 1 + jax.random.randint(jax.random.fold_in(own_key, 4), shape, 0, 1 << 30) % jnp.minimum(start, number_of + 1 - start)
    return jax.random.permutation(jax.random.fold_in(own_key, 2), number_of)[grade].astype(jnp.int32)


def scatter_about(own_key, dims, width, limit, split=(), dtype=jnp.bfloat16):
    entries = jax.random.normal(own_key, dims, jnp.float32) * width
    if len(split) > 0:
        entries = shard_levels(own_key, dims, split, -0.22, 0.18) * entries
    return jnp.clip(entries, min=-limit, max=limit).astype(dtype)


def setup_inputs(seed: int = 0) -> dict:
    seeds = jax.random.split(jax.random.key(seed), 6)
    return {
        "features": scatter_about(seeds[0], (TOKENS, D), 1.0, 6.0, ((0, 16), (1, 32))),
        "key_table": scatter_about(seeds[1], (EXPERTS, D), D ** -0.5, 0.1875, ((0, 16), (1, 32))),
        "value_table": scatter_about(seeds[2], (EXPERTS, D), 1.0, 6.0, ((0, 16), (1, 32))),
        "chosen": plant(ranked_wide(seeds[3], (TOKENS, HEADS, TOPK), EXPERTS, 2), jax.random.fold_in(seeds[3], 3), 0, EXPERTS - 1).astype(jnp.int32),
        "scores": scatter_about(seeds[4], (TOKENS, HEADS, TOPK), 2.0, 8.0, ((0, 16),), jnp.float32),
    }


def reference(features, key_table, value_table, chosen, scores):
    gate_weights = jax.nn.softmax(scores, axis=-1)
    block_count = TOKENS // TOK_DEV

    def per_block(block_data):
        block_tokens, block_rows, block_gates = block_data
        flat_rows = block_rows.reshape(-1).astype(jnp.int32)
        key_rows = jnp.take(key_table, flat_rows, axis=0).reshape(TOK_DEV, HEADS * TOPK, D).astype(jnp.float32)
        products = jnp.einsum("tjd,td->tj", key_rows, block_tokens.astype(jnp.float32), precision=lax.Precision.HIGHEST)
        row_weights = (block_gates.reshape(TOK_DEV, HEADS * TOPK) * jax.nn.gelu(products, approximate=False)).astype(jnp.bfloat16)
        value_rows = jnp.take(value_table, flat_rows, axis=0).reshape(TOK_DEV, HEADS * TOPK, D).astype(jnp.float32)
        summed = jnp.einsum("tj,tjd->td", row_weights.astype(jnp.float32), value_rows, precision=lax.Precision.HIGHEST)
        return summed.astype(jnp.bfloat16)

    outputs = lax.map(per_block, (features.reshape(block_count, TOK_DEV, D),
                                  chosen.reshape(block_count, TOK_DEV, HEADS, TOPK),
                                  gate_weights.reshape(block_count, TOK_DEV, HEADS, TOPK)))
    return outputs.reshape(TOKENS, D)
```

```python
import functools

import jax
import jax.numpy as jnp
from jax import lax
from jax.experimental import pallas as pl
from jax.experimental.pallas import tpu as pltpu
from jax.sharding import PartitionSpec as P

LANES = 128
CORES = 2
PITCH_PAD = 4
GROUP = 4
UNROLL = 16
MESH = pl.DeviceIdType.MESH


def matmul_nt(left, right):
    return lax.dot_general(
        left, right, (((1,), (1,)), ((), ())), preferred_element_type=jnp.float32
    )


def kernel(
    ep_size,
    z_size,
    features_hbm,
    key_hbm,
    value_hbm,
    chosen_hbm,
    scores_hbm,
    out_ref,
    feature_parts,
    features,
    chosen,
    scores,
    picks,
    gates,
    key,
    value,
    dense_even,
    dense_odd,
    partial,
    landed,
    weights,
    spread,
    summed,
    out_landed,
    local_sem,
    table_send,
    table_recv,
    feature_send,
    feature_recv,
    pick_send,
    pick_recv,
    gate_send,
    gate_recv,
    part_send,
    part_recv,
    weight_send,
    weight_recv,
    out_send,
    out_recv,
):
    my_ep = lax.axis_index("ep")
    my_tp = lax.axis_index("tp")
    my_z = my_tp // CORES
    my_core = my_tp % CORES
    other_core = 1 - my_core
    partner = my_z * CORES + other_core
    width = features_hbm.shape[1]
    own_tokens, heads, top = chosen_hbm.shape
    per_token = heads * top
    own_pairs = own_tokens // 2
    half_rows = key.shape[1]
    blocks = half_rows // LANES
    chunk_tokens = GROUP * own_tokens
    pitch = chunk_tokens + PITCH_PAD
    chunks = ep_size // GROUP

    def ep_at(step):
        return lax.rem(my_ep + step, ep_size)

    def z_at(step):
        return lax.rem(my_z + step, z_size)

    def tokens_of(index):
        return pl.ds(pl.multiple_of(index * own_tokens, own_tokens), own_tokens)

    def pairs_of(index):
        return pl.ds(pl.multiple_of(index * own_pairs, own_pairs), own_pairs)

    own_features = feature_parts.at[my_core, tokens_of(my_ep)]
    small = (
        (features_hbm, own_features),
        (chosen_hbm, chosen),
        (scores_hbm, scores),
    )
    small_copies = []
    for number, (source, target) in enumerate(small):
        copy = pltpu.make_async_copy(source, target, local_sem.at[number])
        copy.start()
        small_copies.append(copy)
    half_of = pl.ds(pl.multiple_of(my_core * half_rows, half_rows), half_rows)
    other_half = pl.ds(pl.multiple_of(other_core * half_rows, half_rows), half_rows)
    my_width = pl.ds(pl.multiple_of(my_core * width, width), width)
    table_copies = []
    for number, (source, target) in enumerate(((key_hbm, key), (value_hbm, value))):
        copy = pltpu.make_async_copy(
            source.at[:, half_of], target.at[my_width, :], local_sem.at[3 + number]
        )
        copy.start()
        table_copies.append(copy)

    barrier = pltpu.get_barrier_semaphore()

    def greet(ep, tp):
        pl.semaphore_signal(barrier, inc=1, device_id=(ep, tp), device_id_type=MESH)

    for step in range(1, z_size):
        greet(my_ep, z_at(step) * CORES + my_core)
    for step in range(1, ep_size):
        greet(ep_at(step), my_tp)
        greet(ep_at(step), partner)
    greet(my_ep, partner)

    for copy in small_copies:
        copy.wait()

    def packed(pieces):
        flat = jnp.concatenate(pieces, axis=1)
        return jnp.concatenate([flat[:own_pairs], flat[own_pairs:]], axis=1)

    picks[pairs_of(my_ep), :] = packed([chosen[:, head, :] for head in range(heads)])
    gate_pieces = []
    for head in range(heads):
        logits = scores[:, head, :]
        powers = jnp.exp(logits - jnp.max(logits, axis=1, keepdims=True))
        gate_pieces.append(powers / jnp.sum(powers, axis=1, keepdims=True))

    @pl.when(my_ep == my_z)
    def _():
        gates[...] = packed(gate_pieces)

    pl.semaphore_wait(barrier, z_size - 1 + CORES * (ep_size - 1) + 1)

    def remote(source, target, send, recv, ep, tp):
        return pltpu.make_async_remote_copy(
            src_ref=source,
            dst_ref=target,
            send_sem=send,
            recv_sem=recv,
            device_id=(ep, tp),
            device_id_type=MESH,
        )

    def pick_copy(step, owner):
        slot = picks.at[pairs_of(owner)]
        return remote(
            slot, slot, pick_send.at[step - 1], pick_recv.at[step - 1], ep_at(step), my_tp
        )

    def feature_copy(step, owner, source_core, cross):
        slot = feature_parts.at[source_core, tokens_of(owner)]
        return remote(
            slot,
            slot,
            feature_send.at[cross, step],
            feature_recv.at[cross, step],
            ep_at(step),
            partner if cross else my_tp,
        )

    def gate_copy(step):
        return remote(
            gates, gates, gate_send.at[step - 1], gate_recv.at[0], ep_at(step), my_tp
        )

    def table_copy(number):
        source, target = ((key_hbm, key), (value_hbm, value))[number]
        return remote(
            source.at[:, other_half],
            target.at[my_width, :],
            table_send.at[number],
            table_recv.at[number],
            my_ep,
            partner,
        )

    for step in range(1, ep_size):
        feature_copy(step, my_ep, my_core, 0).start()
        feature_copy(step, my_ep, my_core, 1).start()
        pick_copy(step, my_ep).start()
    feature_copy(0, my_ep, my_core, 1).start()
    table_copy(0).start()

    @pl.when(my_ep == my_z)
    def _():
        for step in range(1, ep_size):
            gate_copy(step).start()

    table_copy(1).start()

    def source_ep(step):
        return lax.rem(my_ep + ep_size - step, ep_size)

    for step in range(1, ep_size):
        feature_copy(step, source_ep(step), my_core, 0).wait_recv()
    for step in range(ep_size):
        feature_copy(step, source_ep(step), other_core, 1).wait_recv()
    features[...] = jnp.concatenate([feature_parts[0], feature_parts[1]], axis=1)
    for step in range(1, ep_size):
        pick_copy(step, source_ep(step)).wait_recv()
    table_copies[0].wait()

    def table_landed(number):
        target = (key, value)[number]
        other_width = pl.ds(pl.multiple_of(other_core * width, width), width)
        return remote(
            (key_hbm, value_hbm)[number].at[:, other_half],
            target.at[other_width, :],
            table_send.at[number],
            table_recv.at[number],
            my_ep,
            partner,
        )

    table_landed(0).wait_recv()

    first_row = (my_ep * CORES + my_core) * half_rows
    in_first = lax.broadcasted_iota(jnp.int32, (own_pairs, LANES), 1) < per_token

    def far_slice(place):
        half = (place + 1) // 2
        offset = z_size // 2 + jnp.where(place % 2 == 0, half, -half)
        return z_at(offset)

    def part_copy(step, target_z):
        return remote(
            partial.at[target_z],
            landed.at[step - 1],
            part_send.at[step - 1],
            part_recv.at[step - 1],
            my_ep,
            target_z * CORES + my_core,
        )

    steps = blocks // UNROLL

    def dense_step(group, step, target):
        rows = jnp.concatenate(
            [features[tokens_of(far_slice(group * GROUP + inner)), :] for inner in range(GROUP)],
            axis=0,
        )
        columns = key[:, step * UNROLL * LANES : (step + 1) * UNROLL * LANES]
        target[...] = jnp.dot(rows, columns, preferred_element_type=jnp.float32)

    def take_step(step, source, found, wanted):
        for inner in range(GROUP):
            row = wanted[inner]
            lane = row & (LANES - 1)
            block = lax.shift_right_arithmetic(row, 7)
            first = inner * own_tokens
            for offset in range(UNROLL):
                columns = slice(offset * LANES, (offset + 1) * LANES)
                upper = jnp.take_along_axis(
                    source[first : first + own_pairs, columns], lane, axis=1
                )
                lower = jnp.take_along_axis(
                    source[first + own_pairs : first + own_tokens, columns], lane, axis=1
                )
                found[inner] = jnp.where(
                    block == step * UNROLL + offset,
                    jnp.where(in_first, upper, lower),
                    found[inner],
                )

    dense_step(0, 0, dense_even)

    def pick_group(group, carry):
        slices = [far_slice(group * GROUP + inner) for inner in range(GROUP)]
        wanted = [picks[pairs_of(index), :] - first_row for index in slices]
        found = [jnp.zeros((own_pairs, LANES), jnp.float32)] * GROUP
        buffers = (dense_even, dense_odd)
        for step in range(steps):
            if step + 1 < steps:
                dense_step(group, step + 1, buffers[(step + 1) % 2])
            else:
                dense_step(jnp.minimum(group + 1, chunks - 1), 0, buffers[(step + 1) % 2])
            take_step(step, buffers[step % 2], found, wanted)
        for inner in range(GROUP):
            partial[slices[inner]] = found[inner]
        for inner in range(GROUP):
            index = slices[inner]
            step = lax.rem(index - my_z + z_size, z_size)

            @pl.when(step != 0)
            def _():
                part_copy(step, index).start()

        return carry

    lax.fori_loop(0, chunks, pick_group, 0)

    @pl.when(my_ep != my_z)
    def _():
        gate_copy(1).wait_recv()

    products = partial[my_z]
    for step in range(1, z_size):
        part_copy(step, my_z).wait_recv()
        products = products + landed[step - 1]
    activated = 0.5 * products * (1.0 + lax.erf(products * (0.5**0.5)))
    weights[my_z] = (gates[...] * activated).astype(jnp.bfloat16).astype(jnp.float32)

    def weight_copy(step, owner):
        slot = weights.at[owner]
        return remote(
            slot,
            slot,
            weight_send.at[step - 1],
            weight_recv.at[step - 1],
            my_ep,
            z_at(step) * CORES + my_core,
        )

    for step in range(1, z_size):
        weight_copy(step, my_z).start()

    table_copies[1].wait()
    table_landed(1).wait_recv()

    def near_offset(place):
        half = (place + 1) // 2
        return jnp.where(place % 2 == 1, half, lax.rem(z_size - half, z_size))

    block_ids = lax.broadcasted_iota(jnp.int32, (blocks, LANES), 0)
    lane_ids = lax.broadcasted_iota(jnp.int32, (LANES, LANES), 0)
    block_first = lax.broadcasted_iota(jnp.int32, (blocks, LANES), 1) < per_token

    def out_copy(token_block, target_core, cross, target_z_slot):
        step = lax.rem(token_block - my_ep + ep_size, ep_size)
        return remote(
            summed.at[target_core, tokens_of(target_z_slot)],
            out_landed.at[cross, step],
            out_send.at[cross, step],
            out_recv.at[cross, step],
            token_block,
            my_z * CORES + target_core,
        )

    def spread_chunk(chunk, carry):
        def spread_slice(inner, inner_carry):
            offset = near_offset(chunk * GROUP + inner)
            index = z_at(offset)

            @pl.when(offset != 0)
            def _():
                weight_copy(z_size - offset, index).wait_recv()

            for row_index in range(own_pairs):
                row = picks[pl.ds(index * own_pairs + row_index, 1), :] - first_row
                weight = weights[index, row_index : row_index + 1, :]
                column_hot = jnp.where(
                    (row & (LANES - 1)) == lane_ids, 1.0, 0.0
                ).astype(jnp.bfloat16)
                block_mask = lax.shift_right_arithmetic(row, 7) == block_ids
                hot = jnp.where(block_mask, weight, 0.0)
                both = jnp.concatenate(
                    [
                        jnp.where(block_first, hot, 0.0).astype(jnp.bfloat16),
                        jnp.where(block_first, 0.0, hot).astype(jnp.bfloat16),
                    ],
                    axis=0,
                )
                placed = matmul_nt(both, column_hot)
                token = inner * own_tokens + row_index
                spread[pl.ds(token, blocks, stride=pitch), :] = placed[:blocks]
                spread[pl.ds(token + own_pairs, blocks, stride=pitch), :] = placed[blocks:]
            return inner_carry

        lax.fori_loop(0, GROUP, spread_slice, 0)
        rows = jnp.concatenate(
            [
                spread[block * pitch : block * pitch + chunk_tokens, :].astype(jnp.bfloat16)
                for block in range(blocks)
            ],
            axis=1,
        )
        total = matmul_nt(rows, value[...])
        for inner in range(GROUP):
            index = z_at(near_offset(chunk * GROUP + inner))
            piece = total[inner * own_tokens : (inner + 1) * own_tokens]
            for target_core in range(CORES):
                summed[target_core, tokens_of(index), :] = piece[
                    :, target_core * width : (target_core + 1) * width
                ]
        for inner in range(GROUP):
            index = z_at(near_offset(chunk * GROUP + inner))

            @pl.when(index != my_ep)
            def _():
                out_copy(index, my_core, 0, index).start()

            out_copy(index, other_core, 1, index).start()
        return carry

    lax.fori_loop(0, chunks, spread_chunk, 0)

    result = summed[my_core, tokens_of(my_ep), :]
    for cross in range(CORES):
        for step in range(1 - cross, ep_size):
            remote(
                summed.at[0, tokens_of(0)],
                out_landed.at[cross, step],
                out_send.at[cross, step],
                out_recv.at[cross, step],
                ep_at(step),
                my_tp,
            ).wait_recv()
            result = result + out_landed[cross, step]
    out_ref[...] = result.astype(out_ref.dtype)

    for step in range(1, ep_size):
        feature_copy(step, my_ep, my_core, 0).wait_send()
        feature_copy(step, my_ep, my_core, 1).wait_send()
        pick_copy(step, my_ep).wait_send()
    feature_copy(0, my_ep, my_core, 1).wait_send()

    @pl.when(my_ep == my_z)
    def _():
        for step in range(1, ep_size):
            gate_copy(step).wait_send()

    for number in range(2):
        table_copy(number).wait_send()
    for step in range(1, z_size):
        part_copy(step, z_at(step)).wait_send()
        weight_copy(step, my_z).wait_send()
    for cross in range(CORES):
        for step in range(1 - cross, ep_size):
            out_copy(
                ep_at(step), other_core if cross else my_core, cross, ep_at(step)
            ).wait_send()


def shards(ep_size, tp_size, features, key_table, value_table, chosen, scores):
    own_tokens, width = features.shape
    _, heads, top = chosen.shape
    half_rows = key_table.shape[0] // CORES
    z_size = tp_size // CORES
    tokens = ep_size * own_tokens
    own_pairs = own_tokens // 2
    blocks = half_rows // LANES
    chunk_tokens = GROUP * own_tokens
    dma = pltpu.SemaphoreType.DMA
    slices = (z_size, own_pairs, LANES)
    return pl.pallas_call(
        functools.partial(kernel, ep_size, z_size),
        out_shape=pltpu.VMEM((own_tokens, width), jnp.bfloat16),
        in_specs=[pl.BlockSpec(memory_space=pl.ANY)] * 5,
        out_specs=pl.BlockSpec(memory_space=pltpu.VMEM),
        scratch_shapes=[
            pltpu.VMEM((CORES, tokens, width), features.dtype),
            pltpu.VMEM((tokens, CORES * width), features.dtype),
            pltpu.VMEM((own_tokens, heads, top), jnp.int32),
            pltpu.VMEM((own_tokens, heads, top), jnp.float32),
            pltpu.VMEM((tokens // 2, LANES), jnp.int32),
            pltpu.VMEM((own_pairs, LANES), jnp.float32),
            pltpu.VMEM((CORES * width, half_rows), key_table.dtype),
            pltpu.VMEM((CORES * width, half_rows), value_table.dtype),
            pltpu.VMEM((chunk_tokens, UNROLL * LANES), jnp.float32),
            pltpu.VMEM((chunk_tokens, UNROLL * LANES), jnp.float32),
            pltpu.VMEM(slices, jnp.float32),
            pltpu.VMEM((z_size - 1,) + slices[1:], jnp.float32),
            pltpu.VMEM(slices, jnp.float32),
            pltpu.VMEM((blocks * (chunk_tokens + PITCH_PAD), LANES), jnp.float32),
            pltpu.VMEM((CORES, tokens, width), jnp.float32),
            pltpu.VMEM((CORES, ep_size, own_tokens, width), jnp.float32),
            dma((5,)),
            dma((2,)),
            dma((2,)),
            dma((CORES, ep_size)),
            dma((CORES, ep_size)),
            dma((ep_size - 1,)),
            dma((ep_size - 1,)),
            dma((ep_size - 1,)),
            dma((1,)),
            dma((z_size - 1,)),
            dma((z_size - 1,)),
            dma((z_size - 1,)),
            dma((z_size - 1,)),
            dma((CORES, ep_size)),
            dma((CORES, ep_size)),
        ],
        compiler_params=pltpu.CompilerParams(collective_id=0, has_side_effects=True),
    )(features, key_table.T, value_table.T, chosen, scores)


def solution(mesh):
    return jax.shard_map(
        functools.partial(shards, mesh.shape["ep"], mesh.shape["tp"]),
        mesh=mesh,
        in_specs=(
            P("ep", "tp"),
            P("ep", "tp"),
            P("ep", "tp"),
            P("ep", None, None),
            P("ep", None, None),
        ),
        out_specs=P("ep", "tp"),
        check_vma=False,
    )
```

```python
import functools

import jax
import jax.numpy as jnp
from jax import lax
from jax.experimental import pallas as pl
from jax.experimental.pallas import tpu as pltpu
from jax.sharding import PartitionSpec as P

LANES = 128
CORES = 2
PITCH_PAD = 4
GROUP = 4
UNROLL = 16
MESH = pl.DeviceIdType.MESH


def matmul_nt(left, right):
    return lax.dot_general(
        left, right, (((1,), (1,)), ((), ())), preferred_element_type=jnp.float32
    )


def kernel(
    ep_size,
    z_size,
    features_hbm,
    key_hbm,
    value_hbm,
    chosen_hbm,
    scores_hbm,
    out_ref,
    feature_parts,
    features,
    chosen,
    scores,
    picks,
    gates,
    key,
    value,
    dense_even,
    dense_odd,
    partial,
    landed,
    weights,
    spread,
    summed,
    out_landed,
    far_sem,
    local_sem,
    table_send,
    table_recv,
    feature_send,
    feature_recv,
    pick_send,
    pick_recv,
    gate_send,
    gate_recv,
    part_send,
    part_recv,
    weight_send,
    weight_recv,
    out_send,
    out_recv,
):
    my_ep = lax.axis_index("ep")
    my_tp = lax.axis_index("tp")
    my_z = my_tp // CORES
    my_core = my_tp % CORES
    other_core = 1 - my_core
    partner = my_z * CORES + other_core
    width = features_hbm.shape[1]
    own_tokens, heads, top = chosen_hbm.shape
    per_token = heads * top
    own_pairs = own_tokens // 2
    half_rows = key.shape[1]
    blocks = half_rows // LANES
    chunk_tokens = GROUP * own_tokens
    pitch = chunk_tokens + PITCH_PAD
    chunks = ep_size // GROUP

    def ep_at(step):
        return lax.rem(my_ep + step, ep_size)

    def z_at(step):
        return lax.rem(my_z + step, z_size)

    def tokens_of(index):
        return pl.ds(pl.multiple_of(index * own_tokens, own_tokens), own_tokens)

    def pairs_of(index):
        return pl.ds(pl.multiple_of(index * own_pairs, own_pairs), own_pairs)

    own_features = feature_parts.at[my_core, tokens_of(my_ep)]
    small = (
        (features_hbm, own_features),
        (chosen_hbm, chosen),
        (scores_hbm, scores),
    )
    small_copies = []
    for number, (source, target) in enumerate(small):
        copy = pltpu.make_async_copy(source, target, local_sem.at[number])
        copy.start()
        small_copies.append(copy)
    half_of = pl.ds(pl.multiple_of(my_core * half_rows, half_rows), half_rows)
    other_half = pl.ds(pl.multiple_of(other_core * half_rows, half_rows), half_rows)
    my_width = pl.ds(pl.multiple_of(my_core * width, width), width)
    table_copies = []
    for number, (source, target) in enumerate(((key_hbm, key), (value_hbm, value))):
        copy = pltpu.make_async_copy(
            source.at[:, half_of], target.at[my_width, :], local_sem.at[3 + number]
        )
        copy.start()
        table_copies.append(copy)

    barrier = pltpu.get_barrier_semaphore()
    reach = z_size // 4

    def greet(ep, tp):
        pl.semaphore_signal(barrier, inc=1, device_id=(ep, tp), device_id_type=MESH)

    for step in range(1, z_size):
        if min(step, z_size - step) <= reach:
            greet(my_ep, z_at(step) * CORES + my_core)
    for step in range(1, ep_size):
        greet(ep_at(step), my_tp)
        greet(ep_at(step), partner)
    greet(my_ep, partner)

    for copy in small_copies:
        copy.wait()

    def packed(pieces):
        flat = jnp.concatenate(pieces, axis=1)
        return jnp.concatenate([flat[:own_pairs], flat[own_pairs:]], axis=1)

    picks[pairs_of(my_ep), :] = packed([chosen[:, head, :] for head in range(heads)])
    gate_pieces = []
    for head in range(heads):
        logits = scores[:, head, :]
        powers = jnp.exp(logits - jnp.max(logits, axis=1, keepdims=True))
        gate_pieces.append(powers / jnp.sum(powers, axis=1, keepdims=True))

    @pl.when(my_ep == my_z)
    def _():
        gates[...] = packed(gate_pieces)

    pl.semaphore_wait(barrier, 2 * reach + CORES * (ep_size - 1) + 1)
    for step in (reach, z_size - reach):
        pl.semaphore_signal(
            far_sem,
            inc=1,
            device_id=(my_ep, z_at(step) * CORES + my_core),
            device_id_type=MESH,
        )

    def remote(source, target, send, recv, ep, tp):
        return pltpu.make_async_remote_copy(
            src_ref=source,
            dst_ref=target,
            send_sem=send,
            recv_sem=recv,
            device_id=(ep, tp),
            device_id_type=MESH,
        )

    def pick_copy(step, owner):
        slot = picks.at[pairs_of(owner)]
        return remote(
            slot, slot, pick_send.at[step - 1], pick_recv.at[step - 1], ep_at(step), my_tp
        )

    def feature_copy(step, owner, source_core, cross):
        slot = feature_parts.at[source_core, tokens_of(owner)]
        return remote(
            slot,
            slot,
            feature_send.at[cross, step],
            feature_recv.at[cross, step],
            ep_at(step),
            partner if cross else my_tp,
        )

    def gate_copy(step):
        return remote(
            gates, gates, gate_send.at[step - 1], gate_recv.at[0], ep_at(step), my_tp
        )

    def table_copy(number):
        source, target = ((key_hbm, key), (value_hbm, value))[number]
        return remote(
            source.at[:, other_half],
            target.at[my_width, :],
            table_send.at[number],
            table_recv.at[number],
            my_ep,
            partner,
        )

    for step in range(1, ep_size):
        feature_copy(step, my_ep, my_core, 0).start()
        feature_copy(step, my_ep, my_core, 1).start()
        pick_copy(step, my_ep).start()
    feature_copy(0, my_ep, my_core, 1).start()
    table_copy(0).start()

    @pl.when(my_ep == my_z)
    def _():
        for step in range(1, ep_size):
            gate_copy(step).start()

    def source_ep(step):
        return lax.rem(my_ep + ep_size - step, ep_size)

    for step in range(1, ep_size):
        feature_copy(step, source_ep(step), my_core, 0).wait_recv()
    for step in range(ep_size):
        feature_copy(step, source_ep(step), other_core, 1).wait_recv()
    features[...] = jnp.concatenate([feature_parts[0], feature_parts[1]], axis=1)
    for step in range(1, ep_size):
        pick_copy(step, source_ep(step)).wait_recv()
    table_copies[0].wait()

    def table_landed(number):
        target = (key, value)[number]
        other_width = pl.ds(pl.multiple_of(other_core * width, width), width)
        return remote(
            (key_hbm, value_hbm)[number].at[:, other_half],
            target.at[other_width, :],
            table_send.at[number],
            table_recv.at[number],
            my_ep,
            partner,
        )

    table_landed(0).wait_recv()

    first_row = (my_ep * CORES + my_core) * half_rows
    in_first = lax.broadcasted_iota(jnp.int32, (own_pairs, LANES), 1) < per_token

    def far_slice(place):
        half = (place + 1) // 2
        offset = z_size // 2 + jnp.where(place % 2 == 0, half, -half)
        return z_at(offset)

    def part_copy(step, target_z):
        return remote(
            partial.at[target_z],
            landed.at[step - 1],
            part_send.at[step - 1],
            part_recv.at[step - 1],
            my_ep,
            target_z * CORES + my_core,
        )

    steps = blocks // UNROLL

    def dense_step(group, step, target):
        rows = jnp.concatenate(
            [features[tokens_of(far_slice(group * GROUP + inner)), :] for inner in range(GROUP)],
            axis=0,
        )
        columns = key[:, step * UNROLL * LANES : (step + 1) * UNROLL * LANES]
        target[...] = jnp.dot(rows, columns, preferred_element_type=jnp.float32)

    def take_step(step, source, found, wanted):
        for inner in range(GROUP):
            row = wanted[inner]
            lane = row & (LANES - 1)
            block = lax.shift_right_arithmetic(row, 7)
            first = inner * own_tokens
            for offset in range(UNROLL):
                columns = slice(offset * LANES, (offset + 1) * LANES)
                upper = jnp.take_along_axis(
                    source[first : first + own_pairs, columns], lane, axis=1
                )
                lower = jnp.take_along_axis(
                    source[first + own_pairs : first + own_tokens, columns], lane, axis=1
                )
                found[inner] = jnp.where(
                    block == step * UNROLL + offset,
                    jnp.where(in_first, upper, lower),
                    found[inner],
                )

    dense_step(0, 0, dense_even)
    pl.semaphore_wait(far_sem, 2)

    def pick_group(group, carry):
        slices = [far_slice(group * GROUP + inner) for inner in range(GROUP)]
        wanted = [picks[pairs_of(index), :] - first_row for index in slices]
        found = [jnp.zeros((own_pairs, LANES), jnp.float32)] * GROUP
        buffers = (dense_even, dense_odd)
        for step in range(steps):
            if step + 1 < steps:
                dense_step(group, step + 1, buffers[(step + 1) % 2])
            else:
                dense_step(jnp.minimum(group + 1, chunks - 1), 0, buffers[(step + 1) % 2])
            take_step(step, buffers[step % 2], found, wanted)
        for inner in range(GROUP):
            partial[slices[inner]] = found[inner]
        for inner in range(GROUP):
            index = slices[inner]
            step = lax.rem(index - my_z + z_size, z_size)

            @pl.when(step != 0)
            def _():
                part_copy(step, index).start()

        return carry

    lax.fori_loop(0, chunks, pick_group, 0)
    table_copy(1).start()

    @pl.when(my_ep != my_z)
    def _():
        gate_copy(1).wait_recv()

    products = partial[my_z]
    for step in range(1, z_size):
        part_copy(step, my_z).wait_recv()
        products = products + landed[step - 1]
    activated = 0.5 * products * (1.0 + lax.erf(products * (0.5**0.5)))
    weights[my_z] = (gates[...] * activated).astype(jnp.bfloat16)

    def weight_copy(step, owner):
        slot = weights.at[owner]
        return remote(
            slot,
            slot,
            weight_send.at[step - 1],
            weight_recv.at[step - 1],
            my_ep,
            z_at(step) * CORES + my_core,
        )

    for step in range(1, z_size):
        weight_copy(step, my_z).start()

    table_copies[1].wait()
    table_landed(1).wait_recv()

    def near_offset(place):
        half = (place + 1) // 2
        return jnp.where(place % 2 == 1, half, lax.rem(z_size - half, z_size))

    block_ids = lax.broadcasted_iota(jnp.int32, (blocks, LANES), 0)
    lane_ids = lax.broadcasted_iota(jnp.int32, (LANES, LANES), 0)
    block_first = lax.broadcasted_iota(jnp.int32, (blocks, LANES), 1) < per_token

    def out_copy(token_block, target_core, cross, target_z_slot):
        step = lax.rem(token_block - my_ep + ep_size, ep_size)
        return remote(
            summed.at[target_core, tokens_of(target_z_slot)],
            out_landed.at[cross, step],
            out_send.at[cross, step],
            out_recv.at[cross, step],
            token_block,
            my_z * CORES + target_core,
        )

    def spread_chunk(chunk, carry):
        def spread_slice(inner, inner_carry):
            offset = near_offset(chunk * GROUP + inner)
            index = z_at(offset)

            @pl.when(offset != 0)
            def _():
                weight_copy(z_size - offset, index).wait_recv()

            slice_weights = weights[index].astype(jnp.float32)
            for row_index in range(own_pairs):
                row = picks[pl.ds(index * own_pairs + row_index, 1), :] - first_row
                weight = slice_weights[row_index : row_index + 1]
                column_hot = jnp.where(
                    (row & (LANES - 1)) == lane_ids, 1.0, 0.0
                ).astype(jnp.bfloat16)
                block_mask = lax.shift_right_arithmetic(row, 7) == block_ids
                hot = jnp.where(block_mask, weight, 0.0)
                both = jnp.concatenate(
                    [
                        jnp.where(block_first, hot, 0.0).astype(jnp.bfloat16),
                        jnp.where(block_first, 0.0, hot).astype(jnp.bfloat16),
                    ],
                    axis=0,
                )
                placed = matmul_nt(both, column_hot)
                token = inner * own_tokens + row_index
                spread[pl.ds(token, blocks, stride=pitch), :] = placed[:blocks]
                spread[pl.ds(token + own_pairs, blocks, stride=pitch), :] = placed[blocks:]
            return inner_carry

        lax.fori_loop(0, GROUP, spread_slice, 0)
        rows = jnp.concatenate(
            [
                spread[block * pitch : block * pitch + chunk_tokens, :].astype(jnp.bfloat16)
                for block in range(blocks)
            ],
            axis=1,
        )
        total = matmul_nt(rows, value[...])
        for inner in range(GROUP):
            index = z_at(near_offset(chunk * GROUP + inner))
            piece = total[inner * own_tokens : (inner + 1) * own_tokens]
            for target_core in range(CORES):
                summed[target_core, tokens_of(index), :] = piece[
                    :, target_core * width : (target_core + 1) * width
                ]
        for inner in range(GROUP):
            index = z_at(near_offset(chunk * GROUP + inner))

            @pl.when(index != my_ep)
            def _():
                out_copy(index, my_core, 0, index).start()

            out_copy(index, other_core, 1, index).start()
        return carry

    lax.fori_loop(0, chunks, spread_chunk, 0)

    result = summed[my_core, tokens_of(my_ep), :]
    for cross in range(CORES):
        for step in range(1 - cross, ep_size):
            remote(
                summed.at[0, tokens_of(0)],
                out_landed.at[cross, step],
                out_send.at[cross, step],
                out_recv.at[cross, step],
                ep_at(step),
                my_tp,
            ).wait_recv()
            result = result + out_landed[cross, step]
    out_ref[...] = result.astype(out_ref.dtype)

    for step in range(1, ep_size):
        feature_copy(step, my_ep, my_core, 0).wait_send()
        feature_copy(step, my_ep, my_core, 1).wait_send()
        pick_copy(step, my_ep).wait_send()
    feature_copy(0, my_ep, my_core, 1).wait_send()

    @pl.when(my_ep == my_z)
    def _():
        for step in range(1, ep_size):
            gate_copy(step).wait_send()

    for number in range(2):
        table_copy(number).wait_send()
    for step in range(1, z_size):
        part_copy(step, z_at(step)).wait_send()
        weight_copy(step, my_z).wait_send()
    for cross in range(CORES):
        for step in range(1 - cross, ep_size):
            out_copy(
                ep_at(step), other_core if cross else my_core, cross, ep_at(step)
            ).wait_send()


def shards(ep_size, tp_size, features, key_table, value_table, chosen, scores):
    own_tokens, width = features.shape
    _, heads, top = chosen.shape
    half_rows = key_table.shape[0] // CORES
    z_size = tp_size // CORES
    tokens = ep_size * own_tokens
    own_pairs = own_tokens // 2
    blocks = half_rows // LANES
    chunk_tokens = GROUP * own_tokens
    dma = pltpu.SemaphoreType.DMA
    slices = (z_size, own_pairs, LANES)
    return pl.pallas_call(
        functools.partial(kernel, ep_size, z_size),
        out_shape=pltpu.VMEM((own_tokens, width), jnp.bfloat16),
        in_specs=[pl.BlockSpec(memory_space=pl.ANY)] * 5,
        out_specs=pl.BlockSpec(memory_space=pltpu.VMEM),
        scratch_shapes=[
            pltpu.VMEM((CORES, tokens, width), features.dtype),
            pltpu.VMEM((tokens, CORES * width), features.dtype),
            pltpu.VMEM((own_tokens, heads, top), jnp.int32),
            pltpu.VMEM((own_tokens, heads, top), jnp.float32),
            pltpu.VMEM((tokens // 2, LANES), jnp.int32),
            pltpu.VMEM((own_pairs, LANES), jnp.float32),
            pltpu.VMEM((CORES * width, half_rows), key_table.dtype),
            pltpu.VMEM((CORES * width, half_rows), value_table.dtype),
            pltpu.VMEM((chunk_tokens, UNROLL * LANES), jnp.float32),
            pltpu.VMEM((chunk_tokens, UNROLL * LANES), jnp.float32),
            pltpu.VMEM(slices, jnp.float32),
            pltpu.VMEM((z_size - 1,) + slices[1:], jnp.float32),
            pltpu.VMEM(slices, jnp.bfloat16),
            pltpu.VMEM((blocks * (chunk_tokens + PITCH_PAD), LANES), jnp.float32),
            pltpu.VMEM((CORES, tokens, width), jnp.float32),
            pltpu.VMEM((CORES, ep_size, own_tokens, width), jnp.float32),
            pltpu.SemaphoreType.REGULAR,
            dma((5,)),
            dma((2,)),
            dma((2,)),
            dma((CORES, ep_size)),
            dma((CORES, ep_size)),
            dma((ep_size - 1,)),
            dma((ep_size - 1,)),
            dma((ep_size - 1,)),
            dma((1,)),
            dma((z_size - 1,)),
            dma((z_size - 1,)),
            dma((z_size - 1,)),
            dma((z_size - 1,)),
            dma((CORES, ep_size)),
            dma((CORES, ep_size)),
        ],
        compiler_params=pltpu.CompilerParams(collective_id=0, has_side_effects=True),
    )(features, key_table.T, value_table.T, chosen, scores)


def solution(mesh):
    return jax.shard_map(
        functools.partial(shards, mesh.shape["ep"], mesh.shape["tp"]),
        mesh=mesh,
        in_specs=(
            P("ep", "tp"),
            P("ep", "tp"),
            P("ep", "tp"),
            P("ep", None, None),
            P("ep", None, None),
        ),
        out_specs=P("ep", "tp"),
        check_vma=False,
    )
```

```python
import functools
import math

import jax
import jax.numpy as jnp
from jax import lax
from jax.experimental import pallas as pl
from jax.experimental.pallas import tpu as pltpu
from jax.sharding import PartitionSpec as P

LANES = 128
CORES = 2
PITCH_PAD = 4
GROUP = 4
LAST = 2
UNROLL = 16
MESH = pl.DeviceIdType.MESH


def matmul_nt(left, right):
    return lax.dot_general(
        left, right, (((1,), (1,)), ((), ())), preferred_element_type=jnp.float32
    )


def kernel(
    ep_size,
    z_size,
    features_hbm,
    key_hbm,
    value_hbm,
    chosen_hbm,
    scores_hbm,
    out_ref,
    own_features,
    feature_parts,
    features,
    chosen,
    scores,
    picks,
    gates,
    key,
    value,
    dense_even,
    dense_odd,
    partial,
    landed,
    weights,
    spread,
    summed,
    out_landed,
    far_sem,
    local_sem,
    table_send,
    table_recv,
    feature_send,
    feature_recv,
    pick_send,
    pick_recv,
    gate_send,
    gate_recv,
    part_send,
    part_recv,
    weight_send,
    weight_recv,
    out_send,
    out_recv,
):
    my_ep = lax.axis_index("ep")
    my_tp = lax.axis_index("tp")
    my_z = my_tp // CORES
    my_core = my_tp % CORES
    other_core = 1 - my_core
    partner = my_z * CORES + other_core
    width = features_hbm.shape[1]
    own_tokens, heads, top = chosen_hbm.shape
    per_token = heads * top
    own_pairs = own_tokens // 2
    half_rows = key.shape[1]
    blocks = half_rows // LANES
    chunks = ep_size // GROUP

    side = math.isqrt(ep_size)
    folds = LANES // width
    fold_rows = own_tokens // folds

    def ep_at(step):
        down, across = step // side, step % side
        return lax.rem(my_ep // side + down, side) * side + lax.rem(
            my_ep + across, side
        )

    def source_ep(step):
        down, across = step // side, step % side
        return lax.rem(my_ep // side + side - down, side) * side + lax.rem(
            my_ep + side - across, side
        )

    def hops(step):
        down, across = step // side, step % side
        return min(down, side - down) + min(across, side - across)

    far_first = sorted(range(1, ep_size), key=hops, reverse=True)

    def ep_step(target):
        down = lax.rem(target // side - my_ep // side + side, side)
        return down * side + lax.rem(target - my_ep + ep_size, side)

    def z_at(step):
        return lax.rem(my_z + step, z_size)

    def tokens_of(index):
        return pl.ds(pl.multiple_of(index * own_tokens, own_tokens), own_tokens)

    def pairs_of(index):
        return pl.ds(pl.multiple_of(index * own_pairs, own_pairs), own_pairs)

    small = (
        (features_hbm, own_features),
        (chosen_hbm, chosen),
        (scores_hbm, scores),
    )
    small_copies = []
    for number, (source, target) in enumerate(small):
        copy = pltpu.make_async_copy(source, target, local_sem.at[number])
        copy.start()
        small_copies.append(copy)
    half_of = pl.ds(pl.multiple_of(my_core * half_rows, half_rows), half_rows)
    other_half = pl.ds(pl.multiple_of(other_core * half_rows, half_rows), half_rows)
    my_width = pl.ds(pl.multiple_of(my_core * width, width), width)
    table_copies = []
    for number, (source, target) in enumerate(((key_hbm, key), (value_hbm, value))):
        copy = pltpu.make_async_copy(
            source.at[:, half_of], target.at[my_width, :], local_sem.at[3 + number]
        )
        copy.start()
        table_copies.append(copy)

    barrier = pltpu.get_barrier_semaphore()
    reach = z_size // 4

    def greet(ep, tp):
        pl.semaphore_signal(barrier, inc=1, device_id=(ep, tp), device_id_type=MESH)

    for step in far_first:
        greet(ep_at(step), my_tp)
        greet(ep_at(step), partner)
        if step <= reach:
            greet(my_ep, z_at(reach + 1 - step) * CORES + my_core)
            greet(my_ep, z_at(z_size - reach - 1 + step) * CORES + my_core)
    greet(my_ep, partner)

    for copy in small_copies:
        copy.wait()

    tokens_here = own_features[...].astype(jnp.float32)
    feature_parts[my_core, my_ep] = jnp.concatenate(
        [tokens_here[fold * fold_rows : (fold + 1) * fold_rows] for fold in range(folds)],
        axis=1,
    ).astype(jnp.bfloat16)

    def unfolded(tile):
        return jnp.concatenate(
            [tile[:, fold * width : (fold + 1) * width] for fold in range(folds)], axis=0
        )

    def packed(pieces):
        flat = jnp.concatenate(pieces, axis=1)
        return jnp.concatenate([flat[:own_pairs], flat[own_pairs:]], axis=1)

    picks[pairs_of(my_ep), :] = packed([chosen[:, head, :] for head in range(heads)])
    gate_pieces = []
    for head in range(heads):
        logits = scores[:, head, :]
        powers = jnp.exp(logits - jnp.max(logits, axis=1, keepdims=True))
        gate_pieces.append(powers / jnp.sum(powers, axis=1, keepdims=True))

    @pl.when(my_ep == my_z)
    def _():
        gates[...] = packed(gate_pieces)

    pl.semaphore_wait(barrier, 2 * reach + CORES * (ep_size - 1) + 1)
    for step in (reach, z_size - reach):
        pl.semaphore_signal(
            far_sem,
            inc=1,
            device_id=(my_ep, z_at(step) * CORES + my_core),
            device_id_type=MESH,
        )

    def remote(source, target, send, recv, ep, tp):
        return pltpu.make_async_remote_copy(
            src_ref=source,
            dst_ref=target,
            send_sem=send,
            recv_sem=recv,
            device_id=(ep, tp),
            device_id_type=MESH,
        )

    def pick_copy(step, owner):
        slot = picks.at[pairs_of(owner)]
        return remote(
            slot, slot, pick_send.at[step - 1], pick_recv.at[step - 1], ep_at(step), my_tp
        )

    def feature_copy(step, owner, source_core, cross):
        slot = feature_parts.at[source_core, owner]
        return remote(
            slot,
            slot,
            feature_send.at[cross, step],
            feature_recv.at[cross, step],
            ep_at(step),
            partner if cross else my_tp,
        )

    def gate_copy(step):
        return remote(
            gates, gates, gate_send.at[step - 1], gate_recv.at[0], ep_at(step), my_tp
        )

    def table_copy(number):
        source, target = ((key_hbm, key), (value_hbm, value))[number]
        return remote(
            source.at[:, other_half],
            target.at[my_width, :],
            table_send.at[number],
            table_recv.at[number],
            my_ep,
            partner,
        )

    for step in far_first:
        feature_copy(step, my_ep, my_core, 0).start()
        feature_copy(step, my_ep, my_core, 1).start()
        pick_copy(step, my_ep).start()
    feature_copy(0, my_ep, my_core, 1).start()
    table_copy(0).start()

    @pl.when(my_ep == my_z)
    def _():
        for step in far_first:
            gate_copy(step).start()

    for step in range(1, ep_size):
        feature_copy(step, source_ep(step), my_core, 0).wait_recv()
    for step in range(ep_size):
        feature_copy(step, source_ep(step), other_core, 1).wait_recv()
    for owner in range(ep_size):
        features[owner * own_tokens : (owner + 1) * own_tokens, :] = jnp.concatenate(
            [
                unfolded(feature_parts[core, owner].astype(jnp.float32))
                for core in range(CORES)
            ],
            axis=1,
        ).astype(jnp.bfloat16)
    for step in range(1, ep_size):
        pick_copy(step, source_ep(step)).wait_recv()
    table_copies[0].wait()

    def table_landed(number):
        target = (key, value)[number]
        other_width = pl.ds(pl.multiple_of(other_core * width, width), width)
        return remote(
            (key_hbm, value_hbm)[number].at[:, other_half],
            target.at[other_width, :],
            table_send.at[number],
            table_recv.at[number],
            my_ep,
            partner,
        )

    table_landed(0).wait_recv()

    first_row = (my_ep * CORES + my_core) * half_rows
    in_first = lax.broadcasted_iota(jnp.int32, (own_pairs, LANES), 1) < per_token

    def far_slice(place):
        half = (place + 1) // 2
        offset = z_size // 2 + jnp.where(place % 2 == 0, half, -half)
        return z_at(offset)

    def part_copy(step, target_z):
        return remote(
            partial.at[target_z],
            landed.at[step - 1],
            part_send.at[step - 1],
            part_recv.at[step - 1],
            my_ep,
            target_z * CORES + my_core,
        )

    steps = blocks // UNROLL

    def dense_step(group, step, target):
        rows = jnp.concatenate(
            [features[tokens_of(far_slice(group * GROUP + inner)), :] for inner in range(GROUP)],
            axis=0,
        )
        columns = key[:, step * UNROLL * LANES : (step + 1) * UNROLL * LANES]
        target[...] = jnp.dot(rows, columns, preferred_element_type=jnp.float32)

    def take_step(step, source, found, wanted):
        for inner in range(GROUP):
            row = wanted[inner]
            lane = row & (LANES - 1)
            block = lax.shift_right_arithmetic(row, 7)
            first = inner * own_tokens
            for offset in range(UNROLL):
                columns = slice(offset * LANES, (offset + 1) * LANES)
                upper = jnp.take_along_axis(
                    source[first : first + own_pairs, columns], lane, axis=1
                )
                lower = jnp.take_along_axis(
                    source[first + own_pairs : first + own_tokens, columns], lane, axis=1
                )
                found[inner] = jnp.where(
                    block == step * UNROLL + offset,
                    jnp.where(in_first, upper, lower),
                    found[inner],
                )

    dense_step(0, 0, dense_even)
    pl.semaphore_wait(far_sem, 2)

    def pick_group(group, carry):
        slices = [far_slice(group * GROUP + inner) for inner in range(GROUP)]
        wanted = [picks[pairs_of(index), :] - first_row for index in slices]
        found = [jnp.zeros((own_pairs, LANES), jnp.float32)] * GROUP
        buffers = (dense_even, dense_odd)
        for step in range(steps):
            if step + 1 < steps:
                dense_step(group, step + 1, buffers[(step + 1) % 2])
            else:
                dense_step(jnp.minimum(group + 1, chunks - 1), 0, buffers[(step + 1) % 2])
            take_step(step, buffers[step % 2], found, wanted)
        for inner in range(GROUP):
            partial[slices[inner]] = found[inner]
        for inner in range(GROUP):
            index = slices[inner]
            step = lax.rem(index - my_z + z_size, z_size)

            @pl.when(step != 0)
            def _():
                part_copy(step, index).start()

        return carry

    lax.fori_loop(0, chunks, pick_group, 0)
    table_copy(1).start()

    @pl.when(my_ep != my_z)
    def _():
        gate_copy(1).wait_recv()

    products = partial[my_z]
    for step in range(1, z_size):
        part_copy(step, my_z).wait_recv()
        products = products + landed[step - 1]
    activated = 0.5 * products * (1.0 + lax.erf(products * (0.5**0.5)))
    weights[my_z] = (gates[...] * activated).astype(jnp.bfloat16)

    def weight_copy(step, owner):
        slot = weights.at[owner]
        return remote(
            slot,
            slot,
            weight_send.at[step - 1],
            weight_recv.at[step - 1],
            my_ep,
            z_at(step) * CORES + my_core,
        )

    for step in range(1, z_size):
        weight_copy(step, my_z).start()

    table_copies[1].wait()
    table_landed(1).wait_recv()

    def near_offset(place):
        half = (place + 1) // 2
        return jnp.where(place % 2 == 1, half, lax.rem(z_size - half, z_size))

    block_ids = lax.broadcasted_iota(jnp.int32, (blocks, LANES), 0)
    lane_ids = lax.broadcasted_iota(jnp.int32, (LANES, LANES), 0)
    block_first = lax.broadcasted_iota(jnp.int32, (blocks, LANES), 1) < per_token

    def out_copy(step, target, cross):
        target_core = other_core if cross else my_core
        return remote(
            summed.at[target_core, target],
            out_landed.at[cross, step],
            out_send.at[cross, step],
            out_recv.at[cross, step],
            target,
            my_z * CORES + target_core,
        )

    def spread_chunk(first, size):
        quarter = fold_rows * size
        pitch = folds * quarter + PITCH_PAD

        def spread_slice(inner, carry):
            offset = near_offset(first + inner)
            index = z_at(offset)

            @pl.when(offset != 0)
            def _():
                weight_copy(z_size - offset, index).wait_recv()

            slice_weights = weights[index].astype(jnp.float32)
            for pair in range(own_pairs):
                row = picks[pl.ds(index * own_pairs + pair, 1), :] - first_row
                weight = slice_weights[pair : pair + 1]
                column_hot = jnp.where(
                    (row & (LANES - 1)) == lane_ids, 1.0, 0.0
                ).astype(jnp.bfloat16)
                block_mask = lax.shift_right_arithmetic(row, 7) == block_ids
                hot = jnp.where(block_mask, weight, 0.0)
                both = jnp.concatenate(
                    [
                        jnp.where(block_first, hot, 0.0).astype(jnp.bfloat16),
                        jnp.where(block_first, 0.0, hot).astype(jnp.bfloat16),
                    ],
                    axis=0,
                )
                placed = matmul_nt(both, column_hot)
                for half in range(2):
                    fold, row_in_fold = divmod(half * own_pairs + pair, fold_rows)
                    place = fold * quarter + inner * fold_rows + row_in_fold
                    spread[pl.ds(place, blocks, stride=pitch), :] = placed[
                        half * blocks : (half + 1) * blocks
                    ]
            return carry

        lax.fori_loop(0, size, spread_slice, 0)
        rows = jnp.concatenate(
            [
                spread[block * pitch : block * pitch + folds * quarter, :].astype(
                    jnp.bfloat16
                )
                for block in range(blocks)
            ],
            axis=1,
        )
        total = matmul_nt(rows, value[...])
        targets = [z_at(near_offset(first + inner)) for inner in range(size)]
        for core in range(CORES):
            piece = jnp.concatenate(
                [
                    total[
                        fold * quarter : (fold + 1) * quarter,
                        core * width : (core + 1) * width,
                    ]
                    for fold in range(folds)
                ],
                axis=1,
            )
            for inner in range(size):
                summed[core, targets[inner]] = piece[
                    inner * fold_rows : (inner + 1) * fold_rows
                ]
        for inner in range(size):
            target = targets[inner]
            step = ep_step(target)

            @pl.when(step != 0)
            def _():
                out_copy(step, target, 0).start()

            out_copy(step, target, 1).start()

    def spread_large(chunk, carry):
        spread_chunk(chunk * GROUP, GROUP)
        return carry

    def spread_small(chunk, carry):
        spread_chunk(z_size - GROUP + chunk * LAST, LAST)
        return carry

    lax.fori_loop(0, chunks - 1, spread_large, 0)
    lax.fori_loop(0, GROUP // LAST, spread_small, 0)

    result = summed[my_core, my_ep]
    for cross in range(CORES):
        for step in range(1 - cross, ep_size):
            out_copy(step, my_ep, cross).wait_recv()
            result = result + out_landed[cross, step]
    out_ref[...] = unfolded(result).astype(out_ref.dtype)

    for step in range(1, ep_size):
        feature_copy(step, my_ep, my_core, 0).wait_send()
        feature_copy(step, my_ep, my_core, 1).wait_send()
        pick_copy(step, my_ep).wait_send()
    feature_copy(0, my_ep, my_core, 1).wait_send()

    @pl.when(my_ep == my_z)
    def _():
        for step in range(1, ep_size):
            gate_copy(step).wait_send()

    for number in range(2):
        table_copy(number).wait_send()
    for step in range(1, z_size):
        part_copy(step, z_at(step)).wait_send()
        weight_copy(step, my_z).wait_send()
    for cross in range(CORES):
        for step in range(1 - cross, ep_size):
            out_copy(step, ep_at(step), cross).wait_send()


def shards(ep_size, tp_size, features, key_table, value_table, chosen, scores):
    own_tokens, width = features.shape
    _, heads, top = chosen.shape
    half_rows = key_table.shape[0] // CORES
    z_size = tp_size // CORES
    tokens = ep_size * own_tokens
    own_pairs = own_tokens // 2
    blocks = half_rows // LANES
    chunk_tokens = GROUP * own_tokens
    dma = pltpu.SemaphoreType.DMA
    slices = (z_size, own_pairs, LANES)
    folded = (own_tokens * width // LANES, LANES)
    return pl.pallas_call(
        functools.partial(kernel, ep_size, z_size),
        out_shape=pltpu.VMEM((own_tokens, width), jnp.bfloat16),
        in_specs=[pl.BlockSpec(memory_space=pl.ANY)] * 5,
        out_specs=pl.BlockSpec(memory_space=pltpu.VMEM),
        scratch_shapes=[
            pltpu.VMEM((own_tokens, width), features.dtype),
            pltpu.VMEM((CORES, ep_size) + folded, features.dtype),
            pltpu.VMEM((tokens, CORES * width), features.dtype),
            pltpu.VMEM((own_tokens, heads, top), jnp.int32),
            pltpu.VMEM((own_tokens, heads, top), jnp.float32),
            pltpu.VMEM((tokens // 2, LANES), jnp.int32),
            pltpu.VMEM((own_pairs, LANES), jnp.float32),
            pltpu.VMEM((CORES * width, half_rows), key_table.dtype),
            pltpu.VMEM((CORES * width, half_rows), value_table.dtype),
            pltpu.VMEM((chunk_tokens, UNROLL * LANES), jnp.float32),
            pltpu.VMEM((chunk_tokens, UNROLL * LANES), jnp.float32),
            pltpu.VMEM(slices, jnp.float32),
            pltpu.VMEM((z_size - 1,) + slices[1:], jnp.float32),
            pltpu.VMEM(slices, jnp.bfloat16),
            pltpu.VMEM((blocks * (chunk_tokens + PITCH_PAD), LANES), jnp.float32),
            pltpu.VMEM((CORES, ep_size) + folded, jnp.float32),
            pltpu.VMEM((CORES, ep_size) + folded, jnp.float32),
            pltpu.SemaphoreType.REGULAR,
            dma((5,)),
            dma((2,)),
            dma((2,)),
            dma((CORES, ep_size)),
            dma((CORES, ep_size)),
            dma((ep_size - 1,)),
            dma((ep_size - 1,)),
            dma((ep_size - 1,)),
            dma((1,)),
            dma((z_size - 1,)),
            dma((z_size - 1,)),
            dma((z_size - 1,)),
            dma((z_size - 1,)),
            dma((CORES, ep_size)),
            dma((CORES, ep_size)),
        ],
        compiler_params=pltpu.CompilerParams(collective_id=0, has_side_effects=True),
    )(features, key_table.T, value_table.T, chosen, scores)


def solution(mesh):
    return jax.shard_map(
        functools.partial(shards, mesh.shape["ep"], mesh.shape["tp"]),
        mesh=mesh,
        in_specs=(
            P("ep", "tp"),
            P("ep", "tp"),
            P("ep", "tp"),
            P("ep", None, None),
            P("ep", None, None),
        ),
        out_specs=P("ep", "tp"),
        check_vma=False,
    )
```

```python
import functools
import math

import jax
import jax.numpy as jnp
from jax import lax
from jax.experimental import pallas as pl
from jax.experimental.pallas import tpu as pltpu
from jax.sharding import PartitionSpec as P

LANES = 128
CORES = 2
PITCH_PAD = 4
FIRST_GROUPS = 2
FIRST = 2
GROUP = 4
LAST = 2
CHUNK = 8
UNROLL = 16
MESH = pl.DeviceIdType.MESH


def matmul_nt(left, right):
    return lax.dot_general(
        left, right, (((1,), (1,)), ((), ())), preferred_element_type=jnp.float32
    )


def kernel(
    ep_size,
    z_size,
    features_hbm,
    key_hbm,
    value_hbm,
    chosen_hbm,
    scores_hbm,
    out_ref,
    own_features,
    feature_parts,
    features,
    chosen,
    scores,
    picks,
    gates,
    key,
    value,
    dense_even,
    dense_odd,
    partial,
    landed,
    weights,
    column_hots,
    spread,
    summed,
    out_landed,
    far_sem,
    local_sem,
    table_send,
    table_recv,
    feature_send,
    feature_recv,
    pick_send,
    pick_recv,
    gate_send,
    gate_recv,
    part_send,
    part_recv,
    weight_send,
    weight_recv,
    out_send,
    out_recv,
):
    my_ep = lax.axis_index("ep")
    my_tp = lax.axis_index("tp")
    my_z = my_tp // CORES
    my_core = my_tp % CORES
    other_core = 1 - my_core
    partner = my_z * CORES + other_core
    width = features_hbm.shape[1]
    own_tokens, heads, top = chosen_hbm.shape
    per_token = heads * top
    own_pairs = own_tokens // 2
    half_rows = key.shape[1]
    blocks = half_rows // LANES

    side = math.isqrt(ep_size)
    folds = LANES // width
    fold_rows = own_tokens // folds

    def ep_at(step):
        down, across = step // side, step % side
        return lax.rem(my_ep // side + down, side) * side + lax.rem(
            my_ep + across, side
        )

    def source_ep(step):
        down, across = step // side, step % side
        return lax.rem(my_ep // side + side - down, side) * side + lax.rem(
            my_ep + side - across, side
        )

    def hops(step):
        down, across = step // side, step % side
        return min(down, side - down) + min(across, side - across)

    far_first = sorted(range(1, ep_size), key=hops, reverse=True)

    def ep_step(target):
        down = lax.rem(target // side - my_ep // side + side, side)
        return down * side + lax.rem(target - my_ep + ep_size, side)

    def z_at(step):
        return lax.rem(my_z + step, z_size)

    def tokens_of(index):
        return pl.ds(pl.multiple_of(index * own_tokens, own_tokens), own_tokens)

    def pairs_of(index):
        return pl.ds(pl.multiple_of(index * own_pairs, own_pairs), own_pairs)

    small = (
        (features_hbm, own_features),
        (chosen_hbm, chosen),
        (scores_hbm, scores),
    )
    small_copies = []
    for number, (source, target) in enumerate(small):
        copy = pltpu.make_async_copy(source, target, local_sem.at[number])
        copy.start()
        small_copies.append(copy)
    half_of = pl.ds(pl.multiple_of(my_core * half_rows, half_rows), half_rows)
    other_half = pl.ds(pl.multiple_of(other_core * half_rows, half_rows), half_rows)
    my_width = pl.ds(pl.multiple_of(my_core * width, width), width)
    table_copies = []
    for number, (source, target) in enumerate(((key_hbm, key), (value_hbm, value))):
        copy = pltpu.make_async_copy(
            source.at[:, half_of], target.at[my_width, :], local_sem.at[3 + number]
        )
        copy.start()
        table_copies.append(copy)

    barrier = pltpu.get_barrier_semaphore()
    reach = z_size // 4

    def greet(ep, tp):
        pl.semaphore_signal(barrier, inc=1, device_id=(ep, tp), device_id_type=MESH)

    for step in far_first:
        greet(ep_at(step), my_tp)
        greet(ep_at(step), partner)
        if step <= reach:
            greet(my_ep, z_at(reach + 1 - step) * CORES + my_core)
            greet(my_ep, z_at(z_size - reach - 1 + step) * CORES + my_core)
    greet(my_ep, partner)

    for copy in small_copies:
        copy.wait()

    tokens_here = own_features[...].astype(jnp.float32)
    feature_parts[my_core, my_ep] = jnp.concatenate(
        [tokens_here[fold * fold_rows : (fold + 1) * fold_rows] for fold in range(folds)],
        axis=1,
    ).astype(jnp.bfloat16)

    def unfolded(tile):
        return jnp.concatenate(
            [tile[:, fold * width : (fold + 1) * width] for fold in range(folds)], axis=0
        )

    def packed(pieces):
        flat = jnp.concatenate(pieces, axis=1)
        return jnp.concatenate([flat[:own_pairs], flat[own_pairs:]], axis=1)

    picks[pairs_of(my_ep), :] = packed([chosen[:, head, :] for head in range(heads)])
    gate_pieces = []
    for head in range(heads):
        logits = scores[:, head, :]
        powers = jnp.exp(logits - jnp.max(logits, axis=1, keepdims=True))
        gate_pieces.append(powers / jnp.sum(powers, axis=1, keepdims=True))

    @pl.when(my_ep == my_z)
    def _():
        gates[...] = packed(gate_pieces)

    pl.semaphore_wait(barrier, 2 * reach + CORES * (ep_size - 1) + 1)
    for step in (reach, z_size - reach):
        pl.semaphore_signal(
            far_sem,
            inc=1,
            device_id=(my_ep, z_at(step) * CORES + my_core),
            device_id_type=MESH,
        )

    def remote(source, target, send, recv, ep, tp):
        return pltpu.make_async_remote_copy(
            src_ref=source,
            dst_ref=target,
            send_sem=send,
            recv_sem=recv,
            device_id=(ep, tp),
            device_id_type=MESH,
        )

    def pick_copy(step, owner):
        slot = picks.at[pairs_of(owner)]
        return remote(
            slot, slot, pick_send.at[step - 1], pick_recv.at[step - 1], ep_at(step), my_tp
        )

    def feature_copy(step, owner, source_core, cross):
        slot = feature_parts.at[source_core, owner]
        return remote(
            slot,
            slot,
            feature_send.at[cross, step],
            feature_recv.at[cross, step],
            ep_at(step),
            partner if cross else my_tp,
        )

    def gate_copy(step):
        return remote(
            gates, gates, gate_send.at[step - 1], gate_recv.at[0], ep_at(step), my_tp
        )

    def table_copy(number):
        source, target = ((key_hbm, key), (value_hbm, value))[number]
        return remote(
            source.at[:, other_half],
            target.at[my_width, :],
            table_send.at[number],
            table_recv.at[number],
            my_ep,
            partner,
        )

    for step in far_first:
        feature_copy(step, my_ep, my_core, 0).start()
        feature_copy(step, my_ep, my_core, 1).start()
        pick_copy(step, my_ep).start()
    feature_copy(0, my_ep, my_core, 1).start()
    table_copy(0).start()

    @pl.when(my_ep == my_z)
    def _():
        for step in far_first:
            gate_copy(step).start()

    for step in range(1, ep_size):
        feature_copy(step, source_ep(step), my_core, 0).wait_recv()
    for step in range(ep_size):
        feature_copy(step, source_ep(step), other_core, 1).wait_recv()
    for owner in range(ep_size):
        features[owner * own_tokens : (owner + 1) * own_tokens, :] = jnp.concatenate(
            [
                unfolded(feature_parts[core, owner].astype(jnp.float32))
                for core in range(CORES)
            ],
            axis=1,
        ).astype(jnp.bfloat16)
    for step in range(1, ep_size):
        pick_copy(step, source_ep(step)).wait_recv()
    table_copies[0].wait()

    def table_landed(number):
        target = (key, value)[number]
        other_width = pl.ds(pl.multiple_of(other_core * width, width), width)
        return remote(
            (key_hbm, value_hbm)[number].at[:, other_half],
            target.at[other_width, :],
            table_send.at[number],
            table_recv.at[number],
            my_ep,
            partner,
        )

    table_landed(0).wait_recv()

    first_row = (my_ep * CORES + my_core) * half_rows
    in_first = lax.broadcasted_iota(jnp.int32, (own_pairs, LANES), 1) < per_token

    def far_slice(place):
        half = (place + 1) // 2
        offset = z_size // 2 + jnp.where(place % 2 == 0, half, -half)
        return z_at(offset)

    def part_copy(step, target_z):
        return remote(
            partial.at[target_z],
            landed.at[step - 1],
            part_send.at[step - 1],
            part_recv.at[step - 1],
            my_ep,
            target_z * CORES + my_core,
        )

    steps = blocks // UNROLL

    def dense_step(first, size, step, target):
        rows = jnp.concatenate(
            [features[tokens_of(far_slice(first + inner)), :] for inner in range(size)],
            axis=0,
        )
        columns = key[:, step * UNROLL * LANES : (step + 1) * UNROLL * LANES]
        target[: size * own_tokens, :] = jnp.dot(
            rows, columns, preferred_element_type=jnp.float32
        )

    def take_step(step, source, found, wanted):
        for inner in range(len(wanted)):
            row = wanted[inner]
            lane = row & (LANES - 1)
            block = lax.shift_right_arithmetic(row, 7)
            first = inner * own_tokens
            for offset in range(UNROLL):
                columns = slice(offset * LANES, (offset + 1) * LANES)
                upper = jnp.take_along_axis(
                    source[first : first + own_pairs, columns], lane, axis=1
                )
                lower = jnp.take_along_axis(
                    source[first + own_pairs : first + own_tokens, columns], lane, axis=1
                )
                found[inner] = jnp.where(
                    block == step * UNROLL + offset,
                    jnp.where(in_first, upper, lower),
                    found[inner],
                )

    buffers = (dense_even, dense_odd)

    def pick_group(first, size, next_first, next_size):
        slices = [far_slice(first + inner) for inner in range(size)]
        wanted = [picks[pairs_of(index), :] - first_row for index in slices]
        found = [jnp.zeros((own_pairs, LANES), jnp.float32)] * size
        for step in range(steps):
            if step + 1 < steps:
                dense_step(first, size, step + 1, buffers[(step + 1) % 2])
            else:
                dense_step(next_first, next_size, 0, buffers[(step + 1) % 2])
            take_step(step, buffers[step % 2], found, wanted)
        for inner in range(size):
            partial[slices[inner]] = found[inner]
        for inner in range(size):
            index = slices[inner]
            step = lax.rem(index - my_z + z_size, z_size)

            @pl.when(step != 0)
            def _():
                part_copy(step, index).start()

    dense_step(0, FIRST, 0, dense_even)
    pl.semaphore_wait(far_sem, 2)

    for group in range(FIRST_GROUPS):
        following = (group + 1) * FIRST
        pick_group(
            group * FIRST,
            FIRST,
            following,
            FIRST if group + 1 < FIRST_GROUPS else GROUP,
        )

    def pick_large(group, carry):
        first = FIRST_GROUPS * FIRST + group * GROUP
        pick_group(first, GROUP, jnp.minimum(first + GROUP, z_size - GROUP), GROUP)
        return carry

    lax.fori_loop(0, (z_size - FIRST_GROUPS * FIRST) // GROUP, pick_large, 0)
    table_copy(1).start()

    wide = own_pairs * LANES
    pair_of = lax.shift_right_arithmetic(
        lax.broadcasted_iota(jnp.int32, (own_pairs, wide), 1), 7
    )
    select = jnp.where(
        pair_of == lax.broadcasted_iota(jnp.int32, (own_pairs, wide), 0), 1.0, 0.0
    ).astype(jnp.bfloat16)
    lane_numbers = lax.broadcasted_iota(jnp.int32, (LANES, LANES), 1).astype(jnp.float32)

    def hot_group(group, carry):
        for inner in range(GROUP):
            index = group * GROUP + inner
            lane = (picks[pairs_of(index), :] & (LANES - 1)).astype(jnp.float32)
            wide_lane = jnp.dot(
                lane.T.astype(jnp.bfloat16), select, preferred_element_type=jnp.float32
            )
            for pair in range(own_pairs):
                column = wide_lane[:, pair * LANES : (pair + 1) * LANES]
                column_hots[index, pair] = jnp.where(
                    column == lane_numbers, 1.0, 0.0
                ).astype(jnp.bfloat16)
        return carry

    lax.fori_loop(0, ep_size // GROUP, hot_group, 0)

    @pl.when(my_ep != my_z)
    def _():
        gate_copy(1).wait_recv()

    products = partial[my_z]
    for step in range(1, z_size):
        part_copy(step, my_z).wait_recv()
        products = products + landed[step - 1]
    activated = 0.5 * products * (1.0 + lax.erf(products * (0.5**0.5)))
    weights[my_z] = (gates[...] * activated).astype(jnp.bfloat16)

    def weight_copy(step, owner):
        slot = weights.at[owner]
        return remote(
            slot,
            slot,
            weight_send.at[step - 1],
            weight_recv.at[step - 1],
            my_ep,
            z_at(step) * CORES + my_core,
        )

    for step in range(1, z_size):
        weight_copy(step, my_z).start()

    table_copies[1].wait()
    table_landed(1).wait_recv()

    def near_offset(place):
        half = (place + 1) // 2
        return jnp.where(place % 2 == 1, half, lax.rem(z_size - half, z_size))

    block_ids = lax.broadcasted_iota(jnp.int32, (blocks, LANES), 0)
    block_first = lax.broadcasted_iota(jnp.int32, (blocks, LANES), 1) < per_token

    def out_copy(step, target, cross):
        target_core = other_core if cross else my_core
        return remote(
            summed.at[target_core, target],
            out_landed.at[cross, step],
            out_send.at[cross, step],
            out_recv.at[cross, step],
            target,
            my_z * CORES + target_core,
        )

    quarter = fold_rows * CHUNK
    pitch = folds * quarter + PITCH_PAD

    def spread_group(first, place, size):
        offsets = [near_offset(first + place + inner) for inner in range(size)]
        for offset in offsets:

            @pl.when(offset != 0)
            def _():
                weight_copy(z_size - offset, z_at(offset)).wait_recv()

        for inner in range(size):
            index = z_at(offsets[inner])
            slice_weights = weights[index].astype(jnp.float32)
            for pair in range(own_pairs):
                row = picks[pl.ds(index * own_pairs + pair, 1), :] - first_row
                block_mask = lax.shift_right_arithmetic(row, 7) == block_ids
                hot = jnp.where(block_mask, slice_weights[pair : pair + 1], 0.0)
                both = jnp.concatenate(
                    [
                        jnp.where(block_first, hot, 0.0).astype(jnp.bfloat16),
                        jnp.where(block_first, 0.0, hot).astype(jnp.bfloat16),
                    ],
                    axis=0,
                )
                placed = jnp.dot(
                    both, column_hots[index, pair], preferred_element_type=jnp.float32
                )
                for half in range(2):
                    fold, row_in_fold = divmod(half * own_pairs + pair, fold_rows)
                    target = fold * quarter + (place + inner) * fold_rows + row_in_fold
                    spread[pl.ds(target, blocks, stride=pitch), :] = placed[
                        half * blocks : (half + 1) * blocks
                    ]

    def spread_chunk(first):
        rows = jnp.concatenate(
            [
                spread[block * pitch : block * pitch + folds * quarter, :].astype(
                    jnp.bfloat16
                )
                for block in range(blocks)
            ],
            axis=1,
        )
        total = matmul_nt(rows, value[...])
        targets = [z_at(near_offset(first + inner)) for inner in range(CHUNK)]
        for core in range(CORES):
            piece = jnp.concatenate(
                [
                    total[
                        fold * quarter : (fold + 1) * quarter,
                        core * width : (core + 1) * width,
                    ]
                    for fold in range(folds)
                ],
                axis=1,
            )
            for inner in range(CHUNK):
                summed[core, targets[inner]] = piece[
                    inner * fold_rows : (inner + 1) * fold_rows
                ]
        for inner in range(CHUNK):
            target = targets[inner]
            step = ep_step(target)

            @pl.when(step != 0)
            def _():
                out_copy(step, target, 0).start()

            out_copy(step, target, 1).start()

    def spread_large(first, groups):
        def step(group, carry):
            spread_group(first, group * GROUP, GROUP)
            return carry

        lax.fori_loop(0, groups, step, 0)

    def spread_small(group, carry):
        spread_group(z_size - CHUNK, CHUNK - GROUP + group * LAST, LAST)
        return carry

    def spread_early(chunk, carry):
        spread_large(chunk * CHUNK, CHUNK // GROUP)
        spread_chunk(chunk * CHUNK)
        return carry

    lax.fori_loop(0, z_size // CHUNK - 1, spread_early, 0)
    spread_large(z_size - CHUNK, CHUNK // GROUP - 1)
    lax.fori_loop(0, GROUP // LAST, spread_small, 0)
    spread_chunk(z_size - CHUNK)

    result = summed[my_core, my_ep]
    for cross in range(CORES):
        for step in range(1 - cross, ep_size):
            out_copy(step, my_ep, cross).wait_recv()
            result = result + out_landed[cross, step]
    out_ref[...] = unfolded(result).astype(out_ref.dtype)

    for step in range(1, ep_size):
        feature_copy(step, my_ep, my_core, 0).wait_send()
        feature_copy(step, my_ep, my_core, 1).wait_send()
        pick_copy(step, my_ep).wait_send()
    feature_copy(0, my_ep, my_core, 1).wait_send()

    @pl.when(my_ep == my_z)
    def _():
        for step in range(1, ep_size):
            gate_copy(step).wait_send()

    for number in range(2):
        table_copy(number).wait_send()
    for step in range(1, z_size):
        part_copy(step, z_at(step)).wait_send()
        weight_copy(step, my_z).wait_send()
    for cross in range(CORES):
        for step in range(1 - cross, ep_size):
            out_copy(step, ep_at(step), cross).wait_send()


def shards(ep_size, tp_size, features, key_table, value_table, chosen, scores):
    own_tokens, width = features.shape
    _, heads, top = chosen.shape
    half_rows = key_table.shape[0] // CORES
    z_size = tp_size // CORES
    tokens = ep_size * own_tokens
    own_pairs = own_tokens // 2
    blocks = half_rows // LANES
    chunk_tokens = CHUNK * own_tokens
    dma = pltpu.SemaphoreType.DMA
    slices = (z_size, own_pairs, LANES)
    folded = (own_tokens * width // LANES, LANES)
    return pl.pallas_call(
        functools.partial(kernel, ep_size, z_size),
        out_shape=pltpu.VMEM((own_tokens, width), jnp.bfloat16),
        in_specs=[pl.BlockSpec(memory_space=pl.ANY)] * 5,
        out_specs=pl.BlockSpec(memory_space=pltpu.VMEM),
        scratch_shapes=[
            pltpu.VMEM((own_tokens, width), features.dtype),
            pltpu.VMEM((CORES, ep_size) + folded, features.dtype),
            pltpu.VMEM((tokens, CORES * width), features.dtype),
            pltpu.VMEM((own_tokens, heads, top), jnp.int32),
            pltpu.VMEM((own_tokens, heads, top), jnp.float32),
            pltpu.VMEM((tokens // 2, LANES), jnp.int32),
            pltpu.VMEM((own_pairs, LANES), jnp.float32),
            pltpu.VMEM((CORES * width, half_rows), key_table.dtype),
            pltpu.VMEM((CORES * width, half_rows), value_table.dtype),
            pltpu.VMEM((GROUP * own_tokens, UNROLL * LANES), jnp.float32),
            pltpu.VMEM((GROUP * own_tokens, UNROLL * LANES), jnp.float32),
            pltpu.VMEM(slices, jnp.float32),
            pltpu.VMEM((z_size - 1,) + slices[1:], jnp.float32),
            pltpu.VMEM(slices, jnp.bfloat16),
            pltpu.VMEM((ep_size, own_pairs, LANES, LANES), jnp.bfloat16),
            pltpu.VMEM((blocks * (chunk_tokens + PITCH_PAD), LANES), jnp.float32),
            pltpu.VMEM((CORES, ep_size) + folded, jnp.float32),
            pltpu.VMEM((CORES, ep_size) + folded, jnp.float32),
            pltpu.SemaphoreType.REGULAR,
            dma((5,)),
            dma((2,)),
            dma((2,)),
            dma((CORES, ep_size)),
            dma((CORES, ep_size)),
            dma((ep_size - 1,)),
            dma((ep_size - 1,)),
            dma((ep_size - 1,)),
            dma((1,)),
            dma((z_size - 1,)),
            dma((z_size - 1,)),
            dma((z_size - 1,)),
            dma((z_size - 1,)),
            dma((CORES, ep_size)),
            dma((CORES, ep_size)),
        ],
        compiler_params=pltpu.CompilerParams(collective_id=0, has_side_effects=True),
    )(features, key_table.T, value_table.T, chosen, scores)


def solution(mesh):
    return jax.shard_map(
        functools.partial(shards, mesh.shape["ep"], mesh.shape["tp"]),
        mesh=mesh,
        in_specs=(
            P("ep", "tp"),
            P("ep", "tp"),
            P("ep", "tp"),
            P("ep", None, None),
            P("ep", None, None),
        ),
        out_specs=P("ep", "tp"),
        check_vma=False,
    )
```

```python
import functools
import math

import jax
import jax.numpy as jnp
from jax import lax
from jax.experimental import pallas as pl
from jax.experimental.pallas import tpu as pltpu
from jax.sharding import PartitionSpec as P

LANES = 128
CORES = 2
PITCH_PAD = 4
FIRST_GROUPS = 2
FIRST = 2
GROUP = 4
LAST = 2
CHUNK = 8
UNROLL = 16
MESH = pl.DeviceIdType.MESH


def matmul_nt(left, right):
    return lax.dot_general(
        left, right, (((1,), (1,)), ((), ())), preferred_element_type=jnp.float32
    )


def kernel(
    ep_size,
    z_size,
    features_hbm,
    key_hbm,
    value_hbm,
    chosen_hbm,
    scores_hbm,
    out_ref,
    own_features,
    feature_parts,
    features,
    chosen,
    scores,
    picks,
    gates,
    key,
    value,
    dense_even,
    dense_odd,
    partial,
    landed,
    weights,
    column_hots,
    spread,
    summed,
    out_landed,
    middle_sem,
    far_sem,
    local_sem,
    table_send,
    table_recv,
    feature_send,
    feature_recv,
    pick_send,
    pick_recv,
    gate_send,
    gate_recv,
    part_send,
    part_recv,
    weight_send,
    weight_recv,
    out_send,
    out_recv,
):
    my_ep = lax.axis_index("ep")
    my_tp = lax.axis_index("tp")
    my_z = my_tp // CORES
    my_core = my_tp % CORES
    other_core = 1 - my_core
    partner = my_z * CORES + other_core
    width = features_hbm.shape[1]
    own_tokens, heads, top = chosen_hbm.shape
    per_token = heads * top
    own_pairs = own_tokens // 2
    half_rows = key.shape[1]
    blocks = half_rows // LANES

    side = math.isqrt(ep_size)
    folds = LANES // width
    fold_rows = own_tokens // folds

    def ep_at(step):
        down, across = step // side, step % side
        return lax.rem(my_ep // side + down, side) * side + lax.rem(
            my_ep + across, side
        )

    def source_ep(step):
        down, across = step // side, step % side
        return lax.rem(my_ep // side + side - down, side) * side + lax.rem(
            my_ep + side - across, side
        )

    def hops(step):
        down, across = step // side, step % side
        return min(down, side - down) + min(across, side - across)

    far_first = sorted(range(1, ep_size), key=hops, reverse=True)

    def ep_step(target):
        down = lax.rem(target // side - my_ep // side + side, side)
        return down * side + lax.rem(target - my_ep + ep_size, side)

    def z_at(step):
        return lax.rem(my_z + step, z_size)

    def tokens_of(index):
        return pl.ds(pl.multiple_of(index * own_tokens, own_tokens), own_tokens)

    def pairs_of(index):
        return pl.ds(pl.multiple_of(index * own_pairs, own_pairs), own_pairs)

    small = (
        (features_hbm, own_features),
        (chosen_hbm, chosen),
        (scores_hbm, scores),
    )
    small_copies = []
    for number, (source, target) in enumerate(small):
        copy = pltpu.make_async_copy(source, target, local_sem.at[number])
        copy.start()
        small_copies.append(copy)
    half_of = pl.ds(pl.multiple_of(my_core * half_rows, half_rows), half_rows)
    other_half = pl.ds(pl.multiple_of(other_core * half_rows, half_rows), half_rows)
    my_width = pl.ds(pl.multiple_of(my_core * width, width), width)
    table_copies = []
    for number, (source, target) in enumerate(((key_hbm, key), (value_hbm, value))):
        copy = pltpu.make_async_copy(
            source.at[:, half_of], target.at[my_width, :], local_sem.at[3 + number]
        )
        copy.start()
        table_copies.append(copy)

    barrier = pltpu.get_barrier_semaphore()
    near, middle = z_size // 8, z_size // 4

    def greet(ep, tp):
        pl.semaphore_signal(barrier, inc=1, device_id=(ep, tp), device_id_type=MESH)

    lines = sorted(range(1, side), key=hops, reverse=True)
    for line in lines:
        greet(ep_at(line), my_tp)
        greet(ep_at(line), partner)
        greet(ep_at(line * side), my_tp)
    for step in range(near, 0, -1):
        greet(my_ep, z_at(step) * CORES + my_core)
        greet(my_ep, z_at(z_size - step) * CORES + my_core)
    greet(my_ep, partner)

    for copy in small_copies:
        copy.wait()

    tokens_here = own_features[...].astype(jnp.float32)
    feature_parts[my_ep, my_core] = jnp.concatenate(
        [tokens_here[fold * fold_rows : (fold + 1) * fold_rows] for fold in range(folds)],
        axis=1,
    ).astype(jnp.bfloat16)

    def unfolded(tile):
        return jnp.concatenate(
            [tile[:, fold * width : (fold + 1) * width] for fold in range(folds)], axis=0
        )

    def packed(pieces):
        flat = jnp.concatenate(pieces, axis=1)
        return jnp.concatenate([flat[:own_pairs], flat[own_pairs:]], axis=1)

    picks[pairs_of(my_ep), :] = packed([chosen[:, head, :] for head in range(heads)])
    gate_pieces = []
    for head in range(heads):
        logits = scores[:, head, :]
        powers = jnp.exp(logits - jnp.max(logits, axis=1, keepdims=True))
        gate_pieces.append(powers / jnp.sum(powers, axis=1, keepdims=True))

    @pl.when(my_ep == my_z)
    def _():
        gates[...] = packed(gate_pieces)

    pl.semaphore_wait(barrier, 3 * (side - 1) + 2 * near + 1)

    def tell(semaphore, distance):
        for step in (distance, z_size - distance):
            pl.semaphore_signal(
                semaphore,
                inc=1,
                device_id=(my_ep, z_at(step) * CORES + my_core),
                device_id_type=MESH,
            )

    tell(middle_sem, near)

    def remote(source, target, send, recv, ep, tp):
        return pltpu.make_async_remote_copy(
            src_ref=source,
            dst_ref=target,
            send_sem=send,
            recv_sem=recv,
            device_id=(ep, tp),
            device_id_type=MESH,
        )

    def pick_copy(line, owner):
        slot = picks.at[pairs_of(owner)]
        return remote(
            slot, slot, pick_send.at[0, line], pick_recv.at[0, line], ep_at(line), my_tp
        )

    def feature_copy(line, owner, source_core, cross):
        slot = feature_parts.at[owner, source_core]
        return remote(
            slot,
            slot,
            feature_send.at[cross, line],
            feature_recv.at[cross, line],
            ep_at(line),
            partner if cross else my_tp,
        )

    def row_copies(line, owner):
        row = owner // side
        row_pairs = side * own_pairs
        copies = []
        for slot, send, recv in (
            (
                feature_parts.at[pl.ds(row * side, side)],
                feature_send.at[CORES, line],
                feature_recv.at[CORES, line],
            ),
            (
                picks.at[pl.ds(pl.multiple_of(row * row_pairs, row_pairs), row_pairs)],
                pick_send.at[1, line],
                pick_recv.at[1, line],
            ),
        ):
            copies.append(remote(slot, slot, send, recv, ep_at(line * side), my_tp))
        return copies

    def gate_copy(step):
        return remote(
            gates, gates, gate_send.at[step - 1], gate_recv.at[0], ep_at(step), my_tp
        )

    def table_copy(number):
        source, target = ((key_hbm, key), (value_hbm, value))[number]
        return remote(
            source.at[:, other_half],
            target.at[my_width, :],
            table_send.at[number],
            table_recv.at[number],
            my_ep,
            partner,
        )

    for line in lines:
        feature_copy(line, my_ep, my_core, 0).start()
        feature_copy(line, my_ep, my_core, 1).start()
        pick_copy(line, my_ep).start()
    feature_copy(0, my_ep, my_core, 1).start()
    table_copy(0).start()

    feature_copy(0, my_ep, other_core, 1).wait_recv()
    for line in lines:
        feature_copy(line, source_ep(line), my_core, 0).wait_recv()
        feature_copy(line, source_ep(line), other_core, 1).wait_recv()
        pick_copy(line, source_ep(line)).wait_recv()
    for line in lines:
        for copy in row_copies(line, my_ep):
            copy.start()
    pl.semaphore_wait(middle_sem, 2)
    tell(far_sem, middle)
    for line in lines:
        for copy in row_copies(line, source_ep(line * side)):
            copy.wait_recv()
    for owner in range(ep_size):
        features[owner * own_tokens : (owner + 1) * own_tokens, :] = jnp.concatenate(
            [
                unfolded(feature_parts[owner, core].astype(jnp.float32))
                for core in range(CORES)
            ],
            axis=1,
        ).astype(jnp.bfloat16)
    table_copies[0].wait()

    def table_landed(number):
        target = (key, value)[number]
        other_width = pl.ds(pl.multiple_of(other_core * width, width), width)
        return remote(
            (key_hbm, value_hbm)[number].at[:, other_half],
            target.at[other_width, :],
            table_send.at[number],
            table_recv.at[number],
            my_ep,
            partner,
        )

    table_landed(0).wait_recv()

    first_row = (my_ep * CORES + my_core) * half_rows
    in_first = lax.broadcasted_iota(jnp.int32, (own_pairs, LANES), 1) < per_token

    def far_slice(place):
        half = (place + 1) // 2
        offset = z_size // 2 + jnp.where(place % 2 == 0, half, -half)
        return z_at(offset)

    def part_copy(step, target_z):
        return remote(
            partial.at[target_z],
            landed.at[step - 1],
            part_send.at[step - 1],
            part_recv.at[step - 1],
            my_ep,
            target_z * CORES + my_core,
        )

    steps = blocks // UNROLL

    def dense_step(first, size, step, target):
        rows = jnp.concatenate(
            [features[tokens_of(far_slice(first + inner)), :] for inner in range(size)],
            axis=0,
        )
        columns = key[:, step * UNROLL * LANES : (step + 1) * UNROLL * LANES]
        target[: size * own_tokens, :] = jnp.dot(
            rows, columns, preferred_element_type=jnp.float32
        )

    def take_step(step, source, found, wanted):
        for inner in range(len(wanted)):
            row = wanted[inner]
            lane = row & (LANES - 1)
            block = lax.shift_right_arithmetic(row, 7)
            first = inner * own_tokens
            for offset in range(UNROLL):
                columns = slice(offset * LANES, (offset + 1) * LANES)
                upper = jnp.take_along_axis(
                    source[first : first + own_pairs, columns], lane, axis=1
                )
                lower = jnp.take_along_axis(
                    source[first + own_pairs : first + own_tokens, columns], lane, axis=1
                )
                found[inner] = jnp.where(
                    block == step * UNROLL + offset,
                    jnp.where(in_first, upper, lower),
                    found[inner],
                )

    buffers = (dense_even, dense_odd)

    def pick_group(first, size, next_first, next_size):
        slices = [far_slice(first + inner) for inner in range(size)]
        wanted = [picks[pairs_of(index), :] - first_row for index in slices]
        found = [jnp.zeros((own_pairs, LANES), jnp.float32)] * size
        for step in range(steps):
            if step + 1 < steps:
                dense_step(first, size, step + 1, buffers[(step + 1) % 2])
            else:
                dense_step(next_first, next_size, 0, buffers[(step + 1) % 2])
            take_step(step, buffers[step % 2], found, wanted)
        for inner in range(size):
            partial[slices[inner]] = found[inner]
        for inner in range(size):
            index = slices[inner]
            step = lax.rem(index - my_z + z_size, z_size)

            @pl.when(step != 0)
            def _():
                part_copy(step, index).start()

    dense_step(0, FIRST, 0, dense_even)
    pl.semaphore_wait(far_sem, 2)

    for group in range(FIRST_GROUPS):
        following = (group + 1) * FIRST
        pick_group(
            group * FIRST,
            FIRST,
            following,
            FIRST if group + 1 < FIRST_GROUPS else GROUP,
        )

    @pl.when(my_ep == my_z)
    def _():
        for step in far_first:
            gate_copy(step).start()

    def pick_large(group, carry):
        first = FIRST_GROUPS * FIRST + group * GROUP
        pick_group(first, GROUP, jnp.minimum(first + GROUP, z_size - GROUP), GROUP)
        return carry

    lax.fori_loop(0, (z_size - FIRST_GROUPS * FIRST) // GROUP, pick_large, 0)
    table_copy(1).start()

    wide = own_pairs * LANES
    pair_of = lax.shift_right_arithmetic(
        lax.broadcasted_iota(jnp.int32, (own_pairs, wide), 1), 7
    )
    select = jnp.where(
        pair_of == lax.broadcasted_iota(jnp.int32, (own_pairs, wide), 0), 1.0, 0.0
    ).astype(jnp.bfloat16)
    lane_numbers = lax.broadcasted_iota(jnp.int32, (LANES, LANES), 1).astype(jnp.float32)

    def hot_group(group, carry):
        for inner in range(GROUP):
            index = group * GROUP + inner
            lane = (picks[pairs_of(index), :] & (LANES - 1)).astype(jnp.float32)
            wide_lane = jnp.dot(
                lane.T.astype(jnp.bfloat16), select, preferred_element_type=jnp.float32
            )
            for pair in range(own_pairs):
                column = wide_lane[:, pair * LANES : (pair + 1) * LANES]
                column_hots[index, pair] = jnp.where(
                    column == lane_numbers, 1.0, 0.0
                ).astype(jnp.bfloat16)
        return carry

    lax.fori_loop(0, ep_size // GROUP, hot_group, 0)

    @pl.when(my_ep != my_z)
    def _():
        gate_copy(1).wait_recv()

    products = partial[my_z]
    for step in range(1, z_size):
        part_copy(step, my_z).wait_recv()
        products = products + landed[step - 1]
    activated = 0.5 * products * (1.0 + lax.erf(products * (0.5**0.5)))
    weights[my_z] = (gates[...] * activated).astype(jnp.bfloat16)

    def weight_copy(step, owner):
        slot = weights.at[owner]
        return remote(
            slot,
            slot,
            weight_send.at[step - 1],
            weight_recv.at[step - 1],
            my_ep,
            z_at(step) * CORES + my_core,
        )

    for step in range(1, z_size):
        weight_copy(step, my_z).start()

    table_copies[1].wait()
    table_landed(1).wait_recv()

    def near_offset(place):
        half = (place + 1) // 2
        return jnp.where(place % 2 == 1, half, lax.rem(z_size - half, z_size))

    block_ids = lax.broadcasted_iota(jnp.int32, (blocks, LANES), 0)
    block_first = lax.broadcasted_iota(jnp.int32, (blocks, LANES), 1) < per_token

    def out_copy(step, target, cross):
        target_core = other_core if cross else my_core
        return remote(
            summed.at[target_core, target],
            out_landed.at[cross, step],
            out_send.at[cross, step],
            out_recv.at[cross, step],
            target,
            my_z * CORES + target_core,
        )

    quarter = fold_rows * CHUNK
    pitch = folds * quarter + PITCH_PAD

    def spread_group(first, place, size):
        offsets = [near_offset(first + place + inner) for inner in range(size)]
        for offset in offsets:

            @pl.when(offset != 0)
            def _():
                weight_copy(z_size - offset, z_at(offset)).wait_recv()

        for inner in range(size):
            index = z_at(offsets[inner])
            slice_weights = weights[index].astype(jnp.float32)
            for pair in range(own_pairs):
                row = picks[pl.ds(index * own_pairs + pair, 1), :] - first_row
                block_mask = lax.shift_right_arithmetic(row, 7) == block_ids
                hot = jnp.where(block_mask, slice_weights[pair : pair + 1], 0.0)
                both = jnp.concatenate(
                    [
                        jnp.where(block_first, hot, 0.0).astype(jnp.bfloat16),
                        jnp.where(block_first, 0.0, hot).astype(jnp.bfloat16),
                    ],
                    axis=0,
                )
                placed = jnp.dot(
                    both, column_hots[index, pair], preferred_element_type=jnp.float32
                )
                for half in range(2):
                    fold, row_in_fold = divmod(half * own_pairs + pair, fold_rows)
                    target = fold * quarter + (place + inner) * fold_rows + row_in_fold
                    spread[pl.ds(target, blocks, stride=pitch), :] = placed[
                        half * blocks : (half + 1) * blocks
                    ]

    def spread_chunk(first):
        rows = jnp.concatenate(
            [
                spread[block * pitch : block * pitch + folds * quarter, :].astype(
                    jnp.bfloat16
                )
                for block in range(blocks)
            ],
            axis=1,
        )
        total = matmul_nt(rows, value[...])
        targets = [z_at(near_offset(first + inner)) for inner in range(CHUNK)]
        for core in range(CORES):
            piece = jnp.concatenate(
                [
                    total[
                        fold * quarter : (fold + 1) * quarter,
                        core * width : (core + 1) * width,
                    ]
                    for fold in range(folds)
                ],
                axis=1,
            )
            for inner in range(CHUNK):
                summed[core, targets[inner]] = piece[
                    inner * fold_rows : (inner + 1) * fold_rows
                ]
        for inner in range(CHUNK):
            target = targets[inner]
            step = ep_step(target)

            @pl.when(step != 0)
            def _():
                out_copy(step, target, 0).start()

            out_copy(step, target, 1).start()

    def spread_large(first, groups):
        def step(group, carry):
            spread_group(first, group * GROUP, GROUP)
            return carry

        lax.fori_loop(0, groups, step, 0)

    def spread_small(group, carry):
        spread_group(z_size - CHUNK, CHUNK - GROUP + group * LAST, LAST)
        return carry

    def spread_early(chunk, carry):
        spread_large(chunk * CHUNK, CHUNK // GROUP)
        spread_chunk(chunk * CHUNK)
        return carry

    lax.fori_loop(0, z_size // CHUNK - 1, spread_early, 0)
    spread_large(z_size - CHUNK, CHUNK // GROUP - 1)
    lax.fori_loop(0, GROUP // LAST, spread_small, 0)
    spread_chunk(z_size - CHUNK)

    result = summed[my_core, my_ep]
    for cross in range(CORES):
        for step in range(1 - cross, ep_size):
            out_copy(step, my_ep, cross).wait_recv()
            result = result + out_landed[cross, step]
    out_ref[...] = unfolded(result).astype(out_ref.dtype)

    for line in lines:
        feature_copy(line, my_ep, my_core, 0).wait_send()
        feature_copy(line, my_ep, my_core, 1).wait_send()
        pick_copy(line, my_ep).wait_send()
        for copy in row_copies(line, my_ep):
            copy.wait_send()
    feature_copy(0, my_ep, my_core, 1).wait_send()

    @pl.when(my_ep == my_z)
    def _():
        for step in range(1, ep_size):
            gate_copy(step).wait_send()

    for number in range(2):
        table_copy(number).wait_send()
    for step in range(1, z_size):
        part_copy(step, z_at(step)).wait_send()
        weight_copy(step, my_z).wait_send()
    for cross in range(CORES):
        for step in range(1 - cross, ep_size):
            out_copy(step, ep_at(step), cross).wait_send()


def shards(ep_size, tp_size, features, key_table, value_table, chosen, scores):
    own_tokens, width = features.shape
    _, heads, top = chosen.shape
    half_rows = key_table.shape[0] // CORES
    z_size = tp_size // CORES
    tokens = ep_size * own_tokens
    own_pairs = own_tokens // 2
    blocks = half_rows // LANES
    chunk_tokens = CHUNK * own_tokens
    dma = pltpu.SemaphoreType.DMA
    side = math.isqrt(ep_size)
    slices = (z_size, own_pairs, LANES)
    folded = (own_tokens * width // LANES, LANES)
    return pl.pallas_call(
        functools.partial(kernel, ep_size, z_size),
        out_shape=pltpu.VMEM((own_tokens, width), jnp.bfloat16),
        in_specs=[pl.BlockSpec(memory_space=pl.ANY)] * 5,
        out_specs=pl.BlockSpec(memory_space=pltpu.VMEM),
        scratch_shapes=[
            pltpu.VMEM((own_tokens, width), features.dtype),
            pltpu.VMEM((ep_size, CORES) + folded, features.dtype),
            pltpu.VMEM((tokens, CORES * width), features.dtype),
            pltpu.VMEM((own_tokens, heads, top), jnp.int32),
            pltpu.VMEM((own_tokens, heads, top), jnp.float32),
            pltpu.VMEM((tokens // 2, LANES), jnp.int32),
            pltpu.VMEM((own_pairs, LANES), jnp.float32),
            pltpu.VMEM((CORES * width, half_rows), key_table.dtype),
            pltpu.VMEM((CORES * width, half_rows), value_table.dtype),
            pltpu.VMEM((GROUP * own_tokens, UNROLL * LANES), jnp.float32),
            pltpu.VMEM((GROUP * own_tokens, UNROLL * LANES), jnp.float32),
            pltpu.VMEM(slices, jnp.float32),
            pltpu.VMEM((z_size - 1,) + slices[1:], jnp.float32),
            pltpu.VMEM(slices, jnp.bfloat16),
            pltpu.VMEM((ep_size, own_pairs, LANES, LANES), jnp.bfloat16),
            pltpu.VMEM((blocks * (chunk_tokens + PITCH_PAD), LANES), jnp.float32),
            pltpu.VMEM((CORES, ep_size) + folded, jnp.float32),
            pltpu.VMEM((CORES, ep_size) + folded, jnp.float32),
            pltpu.SemaphoreType.REGULAR,
            pltpu.SemaphoreType.REGULAR,
            dma((5,)),
            dma((2,)),
            dma((2,)),
            dma((CORES + 1, side)),
            dma((CORES + 1, side)),
            dma((2, side)),
            dma((2, side)),
            dma((ep_size - 1,)),
            dma((1,)),
            dma((z_size - 1,)),
            dma((z_size - 1,)),
            dma((z_size - 1,)),
            dma((z_size - 1,)),
            dma((CORES, ep_size)),
            dma((CORES, ep_size)),
        ],
        compiler_params=pltpu.CompilerParams(collective_id=0, has_side_effects=True),
    )(features, key_table.T, value_table.T, chosen, scores)


def solution(mesh):
    return jax.shard_map(
        functools.partial(shards, mesh.shape["ep"], mesh.shape["tp"]),
        mesh=mesh,
        in_specs=(
            P("ep", "tp"),
            P("ep", "tp"),
            P("ep", "tp"),
            P("ep", None, None),
            P("ep", None, None),
        ),
        out_specs=P("ep", "tp"),
        check_vma=False,
    )
```

```python
import functools
import math

import jax
import jax.numpy as jnp
from jax import lax
from jax.experimental import pallas as pl
from jax.experimental.pallas import tpu as pltpu
from jax.sharding import PartitionSpec as P

LANES = 128
CORES = 2
PITCH_PAD = 4
GROUP = 2
CHUNK = 4
UNROLL = 16
MESH = pl.DeviceIdType.MESH


def matmul_nt(left, right):
    return lax.dot_general(
        left, right, (((1,), (1,)), ((), ())), preferred_element_type=jnp.float32
    )


def kernel(
    ep_size,
    z_size,
    features_hbm,
    key_hbm,
    value_hbm,
    chosen_hbm,
    scores_hbm,
    out_ref,
    own_features,
    feature_parts,
    features,
    chosen,
    scores,
    picks,
    gates,
    key,
    value,
    dense_even,
    dense_odd,
    partial,
    landed,
    weights,
    column_hots,
    spread,
    summed,
    out_landed,
    far_sem,
    local_sem,
    table_send,
    table_recv,
    feature_send,
    feature_recv,
    pick_send,
    pick_recv,
    gate_send,
    gate_recv,
    part_send,
    part_recv,
    weight_send,
    weight_recv,
    out_send,
    out_recv,
):
    my_ep = lax.axis_index("ep")
    my_tp = lax.axis_index("tp")
    my_z = my_tp // CORES
    my_core = my_tp % CORES
    other_core = 1 - my_core
    partner = my_z * CORES + other_core
    width = features_hbm.shape[1]
    own_tokens, heads, top = chosen_hbm.shape
    per_token = heads * top
    own_pairs = own_tokens // 2
    half_rows = key.shape[1]
    blocks = half_rows // LANES

    side = math.isqrt(ep_size)
    folds = LANES // width
    fold_rows = own_tokens // folds

    def ep_at(step):
        down, across = step // side, step % side
        return lax.rem(my_ep // side + down, side) * side + lax.rem(
            my_ep + across, side
        )

    def source_ep(step):
        down, across = step // side, step % side
        return lax.rem(my_ep // side + side - down, side) * side + lax.rem(
            my_ep + side - across, side
        )

    def hops(step):
        down, across = step // side, step % side
        return min(down, side - down) + min(across, side - across)

    far_first = sorted(range(1, ep_size), key=hops, reverse=True)

    def ep_step(target):
        down = lax.rem(target // side - my_ep // side + side, side)
        return down * side + lax.rem(target - my_ep + ep_size, side)

    def z_at(step):
        return lax.rem(my_z + step, z_size)

    def tokens_of(index):
        return pl.ds(pl.multiple_of(index * own_tokens, own_tokens), own_tokens)

    def pairs_of(index):
        return pl.ds(pl.multiple_of(index * own_pairs, own_pairs), own_pairs)

    small = (
        (features_hbm, own_features),
        (chosen_hbm, chosen),
        (scores_hbm, scores),
    )
    small_copies = []
    for number, (source, target) in enumerate(small):
        copy = pltpu.make_async_copy(source, target, local_sem.at[number])
        copy.start()
        small_copies.append(copy)
    half_of = pl.ds(pl.multiple_of(my_core * half_rows, half_rows), half_rows)
    other_half = pl.ds(pl.multiple_of(other_core * half_rows, half_rows), half_rows)
    my_width = pl.ds(pl.multiple_of(my_core * width, width), width)
    table_copies = []
    for number, (source, target) in enumerate(((key_hbm, key), (value_hbm, value))):
        copy = pltpu.make_async_copy(
            source.at[:, half_of], target.at[my_width, :], local_sem.at[3 + number]
        )
        copy.start()
        table_copies.append(copy)

    barrier = pltpu.get_barrier_semaphore()
    reach = z_size // 4

    def greet(ep, tp):
        pl.semaphore_signal(barrier, inc=1, device_id=(ep, tp), device_id_type=MESH)

    for step in far_first:
        greet(ep_at(step), my_tp)
        greet(ep_at(step), partner)
        if step <= reach:
            greet(my_ep, z_at(reach + 1 - step) * CORES + my_core)
            greet(my_ep, z_at(z_size - reach - 1 + step) * CORES + my_core)
    greet(my_ep, partner)

    for copy in small_copies:
        copy.wait()

    tokens_here = own_features[...].astype(jnp.float32)
    feature_parts[my_core, my_ep] = jnp.concatenate(
        [tokens_here[fold * fold_rows : (fold + 1) * fold_rows] for fold in range(folds)],
        axis=1,
    ).astype(jnp.bfloat16)

    def unfolded(tile):
        return jnp.concatenate(
            [tile[:, fold * width : (fold + 1) * width] for fold in range(folds)], axis=0
        )

    def packed(pieces):
        flat = jnp.concatenate(pieces, axis=1)
        return jnp.concatenate([flat[:own_pairs], flat[own_pairs:]], axis=1)

    picks[pairs_of(my_ep), :] = packed([chosen[:, head, :] for head in range(heads)])
    gate_pieces = []
    for head in range(heads):
        logits = scores[:, head, :]
        powers = jnp.exp(logits - jnp.max(logits, axis=1, keepdims=True))
        gate_pieces.append(powers / jnp.sum(powers, axis=1, keepdims=True))

    @pl.when(my_ep == my_z)
    def _():
        gates[...] = packed(gate_pieces)

    pl.semaphore_wait(barrier, 2 * reach + CORES * (ep_size - 1) + 1)
    for step in (reach, z_size - reach):
        pl.semaphore_signal(
            far_sem,
            inc=1,
            device_id=(my_ep, z_at(step) * CORES + my_core),
            device_id_type=MESH,
        )

    def remote(source, target, send, recv, ep, tp):
        return pltpu.make_async_remote_copy(
            src_ref=source,
            dst_ref=target,
            send_sem=send,
            recv_sem=recv,
            device_id=(ep, tp),
            device_id_type=MESH,
        )

    def pick_copy(step, owner):
        slot = picks.at[pairs_of(owner)]
        return remote(
            slot, slot, pick_send.at[step - 1], pick_recv.at[step - 1], ep_at(step), my_tp
        )

    def feature_copy(step, owner, source_core, cross):
        slot = feature_parts.at[source_core, owner]
        return remote(
            slot,
            slot,
            feature_send.at[cross, step],
            feature_recv.at[cross, step],
            ep_at(step),
            partner if cross else my_tp,
        )

    def gate_copy(step):
        return remote(
            gates, gates, gate_send.at[step - 1], gate_recv.at[0], ep_at(step), my_tp
        )

    def table_copy(number):
        source, target = ((key_hbm, key), (value_hbm, value))[number]
        return remote(
            source.at[:, other_half],
            target.at[my_width, :],
            table_send.at[number],
            table_recv.at[number],
            my_ep,
            partner,
        )

    for step in far_first:
        feature_copy(step, my_ep, my_core, 0).start()
        feature_copy(step, my_ep, my_core, 1).start()
        pick_copy(step, my_ep).start()
    feature_copy(0, my_ep, my_core, 1).start()
    table_copy(0).start()

    @pl.when(my_ep == my_z)
    def _():
        for step in far_first:
            gate_copy(step).start()

    for step in range(1, ep_size):
        feature_copy(step, source_ep(step), my_core, 0).wait_recv()
    for step in range(ep_size):
        feature_copy(step, source_ep(step), other_core, 1).wait_recv()
    for owner in range(ep_size):
        features[owner * own_tokens : (owner + 1) * own_tokens, :] = jnp.concatenate(
            [
                unfolded(feature_parts[core, owner].astype(jnp.float32))
                for core in range(CORES)
            ],
            axis=1,
        ).astype(jnp.bfloat16)
    for step in range(1, ep_size):
        pick_copy(step, source_ep(step)).wait_recv()
    table_copies[0].wait()

    def table_landed(number):
        target = (key, value)[number]
        other_width = pl.ds(pl.multiple_of(other_core * width, width), width)
        return remote(
            (key_hbm, value_hbm)[number].at[:, other_half],
            target.at[other_width, :],
            table_send.at[number],
            table_recv.at[number],
            my_ep,
            partner,
        )

    table_landed(0).wait_recv()

    first_row = (my_ep * CORES + my_core) * half_rows
    in_first = lax.broadcasted_iota(jnp.int32, (own_pairs, LANES), 1) < per_token

    def far_slice(place):
        half = (place + 1) // 2
        offset = z_size // 2 + jnp.where(place % 2 == 0, half, -half)
        return z_at(offset)

    def part_copy(step, target_z):
        return remote(
            partial.at[target_z],
            landed.at[step - 1],
            part_send.at[step - 1],
            part_recv.at[step - 1],
            my_ep,
            target_z * CORES + my_core,
        )

    steps = blocks // UNROLL

    def dense_step(first, step, target):
        rows = jnp.concatenate(
            [features[tokens_of(far_slice(first + inner)), :] for inner in range(GROUP)],
            axis=0,
        )
        columns = key[:, step * UNROLL * LANES : (step + 1) * UNROLL * LANES]
        target[...] = jnp.dot(rows, columns, preferred_element_type=jnp.float32)

    def take_step(step, source, found, wanted):
        for inner in range(GROUP):
            row = wanted[inner]
            lane = row & (LANES - 1)
            block = lax.shift_right_arithmetic(row, 7)
            first = inner * own_tokens
            for offset in range(UNROLL):
                columns = slice(offset * LANES, (offset + 1) * LANES)
                upper = jnp.take_along_axis(
                    source[first : first + own_pairs, columns], lane, axis=1
                )
                lower = jnp.take_along_axis(
                    source[first + own_pairs : first + own_tokens, columns], lane, axis=1
                )
                found[inner] = jnp.where(
                    block == step * UNROLL + offset,
                    jnp.where(in_first, upper, lower),
                    found[inner],
                )

    buffers = (dense_even, dense_odd)

    def pick_group(group, carry):
        first = group * GROUP
        following = jnp.minimum(first + GROUP, z_size - GROUP)
        slices = [far_slice(first + inner) for inner in range(GROUP)]
        wanted = [picks[pairs_of(index), :] - first_row for index in slices]
        found = [jnp.zeros((own_pairs, LANES), jnp.float32)] * GROUP
        for step in range(steps):
            if step + 1 < steps:
                dense_step(first, step + 1, buffers[(step + 1) % 2])
            else:
                dense_step(following, 0, buffers[(step + 1) % 2])
            take_step(step, buffers[step % 2], found, wanted)
        for inner in range(GROUP):
            partial[slices[inner]] = found[inner]
        for inner in range(GROUP):
            index = slices[inner]
            step = lax.rem(index - my_z + z_size, z_size)

            @pl.when(step != 0)
            def _():
                part_copy(step, index).start()

        return carry

    dense_step(0, 0, dense_even)
    pl.semaphore_wait(far_sem, 2)
    lax.fori_loop(0, z_size // GROUP, pick_group, 0)
    table_copy(1).start()

    wide = own_pairs * LANES
    pair_of = lax.shift_right_arithmetic(
        lax.broadcasted_iota(jnp.int32, (own_pairs, wide), 1), 7
    )
    select = jnp.where(
        pair_of == lax.broadcasted_iota(jnp.int32, (own_pairs, wide), 0), 1.0, 0.0
    ).astype(jnp.bfloat16)
    lane_numbers = lax.broadcasted_iota(jnp.int32, (LANES, LANES), 1).astype(jnp.float32)

    def hot_group(group, carry):
        for inner in range(GROUP):
            index = group * GROUP + inner
            lane = (picks[pairs_of(index), :] & (LANES - 1)).astype(jnp.float32)
            wide_lane = jnp.dot(
                lane.T.astype(jnp.bfloat16), select, preferred_element_type=jnp.float32
            )
            for pair in range(own_pairs):
                column = wide_lane[:, pair * LANES : (pair + 1) * LANES]
                column_hots[index, pair] = jnp.where(
                    column == lane_numbers, 1.0, 0.0
                ).astype(jnp.bfloat16)
        return carry

    lax.fori_loop(0, ep_size // GROUP, hot_group, 0)

    @pl.when(my_ep != my_z)
    def _():
        gate_copy(1).wait_recv()

    products = partial[my_z]
    for step in range(1, z_size):
        part_copy(step, my_z).wait_recv()
        products = products + landed[step - 1]
    activated = 0.5 * products * (1.0 + lax.erf(products * (0.5**0.5)))
    weights[my_z] = (gates[...] * activated).astype(jnp.bfloat16)

    def weight_copy(step, owner):
        slot = weights.at[owner]
        return remote(
            slot,
            slot,
            weight_send.at[step - 1],
            weight_recv.at[step - 1],
            my_ep,
            z_at(step) * CORES + my_core,
        )

    for step in range(1, z_size):
        weight_copy(step, my_z).start()

    table_copies[1].wait()
    table_landed(1).wait_recv()

    def near_offset(place):
        half = (place + 1) // 2
        return jnp.where(place % 2 == 1, half, lax.rem(z_size - half, z_size))

    block_ids = lax.broadcasted_iota(jnp.int32, (blocks, LANES), 0)
    block_first = lax.broadcasted_iota(jnp.int32, (blocks, LANES), 1) < per_token

    def out_copy(step, target, cross):
        target_core = other_core if cross else my_core
        return remote(
            summed.at[target_core, target],
            out_landed.at[cross, step],
            out_send.at[cross, step],
            out_recv.at[cross, step],
            target,
            my_z * CORES + target_core,
        )

    quarter = fold_rows * CHUNK
    pitch = folds * quarter + PITCH_PAD

    def spread_group(first, place):
        offsets = [near_offset(first + place + inner) for inner in range(GROUP)]
        for offset in offsets:

            @pl.when(offset != 0)
            def _():
                weight_copy(z_size - offset, z_at(offset)).wait_recv()

        for inner in range(GROUP):
            index = z_at(offsets[inner])
            slice_weights = weights[index].astype(jnp.float32)
            for pair in range(own_pairs):
                row = picks[pl.ds(index * own_pairs + pair, 1), :] - first_row
                block_mask = lax.shift_right_arithmetic(row, 7) == block_ids
                hot = jnp.where(block_mask, slice_weights[pair : pair + 1], 0.0)
                both = jnp.concatenate(
                    [
                        jnp.where(block_first, hot, 0.0).astype(jnp.bfloat16),
                        jnp.where(block_first, 0.0, hot).astype(jnp.bfloat16),
                    ],
                    axis=0,
                )
                placed = jnp.dot(
                    both, column_hots[index, pair], preferred_element_type=jnp.float32
                )
                for half in range(2):
                    fold, row_in_fold = divmod(half * own_pairs + pair, fold_rows)
                    target = fold * quarter + (place + inner) * fold_rows + row_in_fold
                    spread[pl.ds(target, blocks, stride=pitch), :] = placed[
                        half * blocks : (half + 1) * blocks
                    ]

    def spread_chunk(first):
        rows = jnp.concatenate(
            [
                spread[block * pitch : block * pitch + folds * quarter, :].astype(
                    jnp.bfloat16
                )
                for block in range(blocks)
            ],
            axis=1,
        )
        total = matmul_nt(rows, value[...])
        targets = [z_at(near_offset(first + inner)) for inner in range(CHUNK)]
        for core in range(CORES):
            piece = jnp.concatenate(
                [
                    total[
                        fold * quarter : (fold + 1) * quarter,
                        core * width : (core + 1) * width,
                    ]
                    for fold in range(folds)
                ],
                axis=1,
            )
            for inner in range(CHUNK):
                summed[core, targets[inner]] = piece[
                    inner * fold_rows : (inner + 1) * fold_rows
                ]
        for inner in range(CHUNK):
            target = targets[inner]
            step = ep_step(target)

            @pl.when(step != 0)
            def _():
                out_copy(step, target, 0).start()

            out_copy(step, target, 1).start()

    def spread_step(chunk, carry):
        def step(group, inner_carry):
            spread_group(chunk * CHUNK, group * GROUP)
            return inner_carry

        lax.fori_loop(0, CHUNK // GROUP, step, 0)
        spread_chunk(chunk * CHUNK)
        return carry

    lax.fori_loop(0, z_size // CHUNK, spread_step, 0)

    result = summed[my_core, my_ep]
    for cross in range(CORES):
        for step in range(1 - cross, ep_size):
            out_copy(step, my_ep, cross).wait_recv()
            result = result + out_landed[cross, step]
    out_ref[...] = unfolded(result).astype(out_ref.dtype)

    for step in range(1, ep_size):
        feature_copy(step, my_ep, my_core, 0).wait_send()
        feature_copy(step, my_ep, my_core, 1).wait_send()
        pick_copy(step, my_ep).wait_send()
    feature_copy(0, my_ep, my_core, 1).wait_send()

    @pl.when(my_ep == my_z)
    def _():
        for step in range(1, ep_size):
            gate_copy(step).wait_send()

    for number in range(2):
        table_copy(number).wait_send()
    for step in range(1, z_size):
        part_copy(step, z_at(step)).wait_send()
        weight_copy(step, my_z).wait_send()
    for cross in range(CORES):
        for step in range(1 - cross, ep_size):
            out_copy(step, ep_at(step), cross).wait_send()


def shards(ep_size, tp_size, features, key_table, value_table, chosen, scores):
    own_tokens, width = features.shape
    _, heads, top = chosen.shape
    half_rows = key_table.shape[0] // CORES
    z_size = tp_size // CORES
    tokens = ep_size * own_tokens
    own_pairs = own_tokens // 2
    blocks = half_rows // LANES
    chunk_tokens = CHUNK * own_tokens
    dma = pltpu.SemaphoreType.DMA
    slices = (z_size, own_pairs, LANES)
    folded = (own_tokens * width // LANES, LANES)
    return pl.pallas_call(
        functools.partial(kernel, ep_size, z_size),
        out_shape=pltpu.VMEM((own_tokens, width), jnp.bfloat16),
        in_specs=[pl.BlockSpec(memory_space=pl.ANY)] * 5,
        out_specs=pl.BlockSpec(memory_space=pltpu.VMEM),
        scratch_shapes=[
            pltpu.VMEM((own_tokens, width), features.dtype),
            pltpu.VMEM((CORES, ep_size) + folded, features.dtype),
            pltpu.VMEM((tokens, CORES * width), features.dtype),
            pltpu.VMEM((own_tokens, heads, top), jnp.int32),
            pltpu.VMEM((own_tokens, heads, top), jnp.float32),
            pltpu.VMEM((tokens // 2, LANES), jnp.int32),
            pltpu.VMEM((own_pairs, LANES), jnp.float32),
            pltpu.VMEM((CORES * width, half_rows), key_table.dtype),
            pltpu.VMEM((CORES * width, half_rows), value_table.dtype),
            pltpu.VMEM((GROUP * own_tokens, UNROLL * LANES), jnp.float32),
            pltpu.VMEM((GROUP * own_tokens, UNROLL * LANES), jnp.float32),
            pltpu.VMEM(slices, jnp.float32),
            pltpu.VMEM((z_size - 1,) + slices[1:], jnp.float32),
            pltpu.VMEM(slices, jnp.bfloat16),
            pltpu.VMEM((ep_size, own_pairs, LANES, LANES), jnp.bfloat16),
            pltpu.VMEM((blocks * (chunk_tokens + PITCH_PAD), LANES), jnp.float32),
            pltpu.VMEM((CORES, ep_size) + folded, jnp.float32),
            pltpu.VMEM((CORES, ep_size) + folded, jnp.float32),
            pltpu.SemaphoreType.REGULAR,
            dma((5,)),
            dma((2,)),
            dma((2,)),
            dma((CORES, ep_size)),
            dma((CORES, ep_size)),
            dma((ep_size - 1,)),
            dma((ep_size - 1,)),
            dma((ep_size - 1,)),
            dma((1,)),
            dma((z_size - 1,)),
            dma((z_size - 1,)),
            dma((z_size - 1,)),
            dma((z_size - 1,)),
            dma((CORES, ep_size)),
            dma((CORES, ep_size)),
        ],
        compiler_params=pltpu.CompilerParams(collective_id=0, has_side_effects=True),
    )(features, key_table.T, value_table.T, chosen, scores)


def solution(mesh):
    return jax.shard_map(
        functools.partial(shards, mesh.shape["ep"], mesh.shape["tp"]),
        mesh=mesh,
        in_specs=(
            P("ep", "tp"),
            P("ep", "tp"),
            P("ep", "tp"),
            P("ep", None, None),
            P("ep", None, None),
        ),
        out_specs=P("ep", "tp"),
        check_vma=False,
    )
```

```python
import functools
import math

import jax
import jax.numpy as jnp
from jax import lax
from jax.experimental import pallas as pl
from jax.experimental.pallas import tpu as pltpu
from jax.sharding import PartitionSpec as P

LANES = 128
CORES = 2
PITCH_PAD = 4
GROUP = 2
CHUNK = 4
UNROLL = 16
MESH = pl.DeviceIdType.MESH


def matmul_nt(left, right):
    return lax.dot_general(
        left, right, (((1,), (1,)), ((), ())), preferred_element_type=jnp.float32
    )


def kernel(
    ep_size,
    z_size,
    features_hbm,
    key_hbm,
    value_hbm,
    chosen_hbm,
    scores_hbm,
    out_ref,
    own_features,
    feature_parts,
    features,
    chosen,
    scores,
    picks,
    gates,
    key,
    value,
    dense_even,
    dense_odd,
    partial,
    landed,
    weights,
    column_hots,
    spread,
    summed,
    out_landed,
    far_sem,
    local_sem,
    table_send,
    table_recv,
    feature_send,
    feature_recv,
    pick_send,
    pick_recv,
    gate_send,
    gate_recv,
    part_send,
    part_recv,
    weight_send,
    weight_recv,
    out_send,
    out_recv,
):
    my_ep = lax.axis_index("ep")
    my_tp = lax.axis_index("tp")
    my_z = my_tp // CORES
    my_core = my_tp % CORES
    other_core = 1 - my_core
    partner = my_z * CORES + other_core
    width = features_hbm.shape[1]
    own_tokens, heads, top = chosen_hbm.shape
    per_token = heads * top
    own_pairs = own_tokens // 2
    half_rows = key.shape[1]
    blocks = half_rows // LANES

    side = math.isqrt(ep_size)
    folds = LANES // width
    fold_rows = own_tokens // folds

    def ep_at(step):
        down, across = step // side, step % side
        return lax.rem(my_ep // side + down, side) * side + lax.rem(
            my_ep + across, side
        )

    def source_ep(step):
        down, across = step // side, step % side
        return lax.rem(my_ep // side + side - down, side) * side + lax.rem(
            my_ep + side - across, side
        )

    def hops(step):
        down, across = step // side, step % side
        return min(down, side - down) + min(across, side - across)

    far_first = sorted(range(1, ep_size), key=hops, reverse=True)

    def ep_step(target):
        down = lax.rem(target // side - my_ep // side + side, side)
        return down * side + lax.rem(target - my_ep + ep_size, side)

    def z_at(step):
        return lax.rem(my_z + step, z_size)

    def tokens_of(index):
        return pl.ds(pl.multiple_of(index * own_tokens, own_tokens), own_tokens)

    def pairs_of(index):
        return pl.ds(pl.multiple_of(index * own_pairs, own_pairs), own_pairs)

    small = (
        (features_hbm, own_features),
        (chosen_hbm, chosen),
        (scores_hbm, scores),
    )
    small_copies = []
    for number, (source, target) in enumerate(small):
        copy = pltpu.make_async_copy(source, target, local_sem.at[number])
        copy.start()
        small_copies.append(copy)
    half_of = pl.ds(pl.multiple_of(my_core * half_rows, half_rows), half_rows)
    other_half = pl.ds(pl.multiple_of(other_core * half_rows, half_rows), half_rows)
    my_width = pl.ds(pl.multiple_of(my_core * width, width), width)
    table_copies = []
    for number, (source, target) in enumerate(((key_hbm, key), (value_hbm, value))):
        copy = pltpu.make_async_copy(
            source.at[:, half_of], target.at[my_width, :], local_sem.at[3 + number]
        )
        copy.start()
        table_copies.append(copy)

    barrier = pltpu.get_barrier_semaphore()
    reach = z_size // 4

    def greet(ep, tp):
        pl.semaphore_signal(barrier, inc=1, device_id=(ep, tp), device_id_type=MESH)

    for step in range(reach, 0, -1):
        greet(my_ep, z_at(step) * CORES + my_core)
        greet(my_ep, z_at(z_size - step) * CORES + my_core)
    for step in far_first:
        greet(ep_at(step), my_tp)
        greet(ep_at(step), partner)
    greet(my_ep, partner)

    for copy in small_copies:
        copy.wait()

    tokens_here = own_features[...].astype(jnp.float32)
    feature_parts[my_core, my_ep] = jnp.concatenate(
        [tokens_here[fold * fold_rows : (fold + 1) * fold_rows] for fold in range(folds)],
        axis=1,
    ).astype(jnp.bfloat16)

    def unfolded(tile):
        return jnp.concatenate(
            [tile[:, fold * width : (fold + 1) * width] for fold in range(folds)], axis=0
        )

    def packed(pieces):
        flat = jnp.concatenate(pieces, axis=1)
        return jnp.concatenate([flat[:own_pairs], flat[own_pairs:]], axis=1)

    picks[pairs_of(my_ep), :] = packed([chosen[:, head, :] for head in range(heads)])
    gate_pieces = []
    for head in range(heads):
        logits = scores[:, head, :]
        powers = jnp.exp(logits - jnp.max(logits, axis=1, keepdims=True))
        gate_pieces.append(powers / jnp.sum(powers, axis=1, keepdims=True))

    @pl.when(my_ep == my_z)
    def _():
        gates[...] = packed(gate_pieces)

    pl.semaphore_wait(barrier, 2 * reach + CORES * (ep_size - 1) + 1)
    for step in (reach, z_size - reach):
        pl.semaphore_signal(
            far_sem,
            inc=1,
            device_id=(my_ep, z_at(step) * CORES + my_core),
            device_id_type=MESH,
        )

    def remote(source, target, send, recv, ep, tp):
        return pltpu.make_async_remote_copy(
            src_ref=source,
            dst_ref=target,
            send_sem=send,
            recv_sem=recv,
            device_id=(ep, tp),
            device_id_type=MESH,
        )

    def pick_copy(step, owner):
        slot = picks.at[pairs_of(owner)]
        return remote(
            slot, slot, pick_send.at[step - 1], pick_recv.at[step - 1], ep_at(step), my_tp
        )

    def feature_copy(step, owner, source_core, cross):
        slot = feature_parts.at[source_core, owner]
        return remote(
            slot,
            slot,
            feature_send.at[cross, step],
            feature_recv.at[cross, step],
            ep_at(step),
            partner if cross else my_tp,
        )

    def gate_copy(step):
        return remote(
            gates, gates, gate_send.at[step - 1], gate_recv.at[0], ep_at(step), my_tp
        )

    def table_copy(number):
        source, target = ((key_hbm, key), (value_hbm, value))[number]
        return remote(
            source.at[:, other_half],
            target.at[my_width, :],
            table_send.at[number],
            table_recv.at[number],
            my_ep,
            partner,
        )

    for step in far_first:
        feature_copy(step, my_ep, my_core, 0).start()
        feature_copy(step, my_ep, my_core, 1).start()
    for step in far_first:
        pick_copy(step, my_ep).start()
    feature_copy(0, my_ep, my_core, 1).start()
    table_copy(0).start()

    @pl.when(my_ep == my_z)
    def _():
        for step in far_first:
            gate_copy(step).start()

    for step in range(1, ep_size):
        feature_copy(step, source_ep(step), my_core, 0).wait_recv()
    for step in range(ep_size):
        feature_copy(step, source_ep(step), other_core, 1).wait_recv()
    for owner in range(ep_size):
        features[owner * own_tokens : (owner + 1) * own_tokens, :] = jnp.concatenate(
            [
                unfolded(feature_parts[core, owner].astype(jnp.float32))
                for core in range(CORES)
            ],
            axis=1,
        ).astype(jnp.bfloat16)
    for step in range(1, ep_size):
        pick_copy(step, source_ep(step)).wait_recv()
    table_copies[0].wait()

    def table_landed(number):
        target = (key, value)[number]
        other_width = pl.ds(pl.multiple_of(other_core * width, width), width)
        return remote(
            (key_hbm, value_hbm)[number].at[:, other_half],
            target.at[other_width, :],
            table_send.at[number],
            table_recv.at[number],
            my_ep,
            partner,
        )

    table_landed(0).wait_recv()

    first_row = (my_ep * CORES + my_core) * half_rows
    in_first = lax.broadcasted_iota(jnp.int32, (own_pairs, LANES), 1) < per_token

    def far_slice(place):
        half = (place + 1) // 2
        offset = z_size // 2 + jnp.where(place % 2 == 0, half, -half)
        return z_at(offset)

    def part_copy(step, target_z):
        return remote(
            partial.at[target_z],
            landed.at[step - 1],
            part_send.at[step - 1],
            part_recv.at[step - 1],
            my_ep,
            target_z * CORES + my_core,
        )

    steps = blocks // UNROLL

    def dense_step(first, step, target):
        rows = jnp.concatenate(
            [features[tokens_of(far_slice(first + inner)), :] for inner in range(GROUP)],
            axis=0,
        )
        columns = key[:, step * UNROLL * LANES : (step + 1) * UNROLL * LANES]
        target[...] = jnp.dot(rows, columns, preferred_element_type=jnp.float32)

    def take_step(step, source, found, wanted):
        for inner in range(GROUP):
            row = wanted[inner]
            lane = row & (LANES - 1)
            block = lax.shift_right_arithmetic(row, 7)
            first = inner * own_tokens
            for offset in range(UNROLL):
                columns = slice(offset * LANES, (offset + 1) * LANES)
                upper = jnp.take_along_axis(
                    source[first : first + own_pairs, columns], lane, axis=1
                )
                lower = jnp.take_along_axis(
                    source[first + own_pairs : first + own_tokens, columns], lane, axis=1
                )
                found[inner] = jnp.where(
                    block == step * UNROLL + offset,
                    jnp.where(in_first, upper, lower),
                    found[inner],
                )

    buffers = (dense_even, dense_odd)

    def pick_group(group, carry):
        first = group * GROUP
        following = jnp.minimum(first + GROUP, z_size - GROUP)
        slices = [far_slice(first + inner) for inner in range(GROUP)]
        wanted = [picks[pairs_of(index), :] - first_row for index in slices]
        found = [jnp.zeros((own_pairs, LANES), jnp.float32)] * GROUP
        for step in range(steps):
            if step + 1 < steps:
                dense_step(first, step + 1, buffers[(step + 1) % 2])
            else:
                dense_step(following, 0, buffers[(step + 1) % 2])
            take_step(step, buffers[step % 2], found, wanted)
        for inner in range(GROUP):
            partial[slices[inner]] = found[inner]
        for inner in range(GROUP):
            index = slices[inner]
            step = lax.rem(index - my_z + z_size, z_size)

            @pl.when(step != 0)
            def _():
                part_copy(step, index).start()

        return carry

    dense_step(0, 0, dense_even)
    pl.semaphore_wait(far_sem, 2)
    lax.fori_loop(0, z_size // GROUP, pick_group, 0)
    table_copy(1).start()

    wide = own_pairs * LANES
    pair_of = lax.shift_right_arithmetic(
        lax.broadcasted_iota(jnp.int32, (own_pairs, wide), 1), 7
    )
    select = jnp.where(
        pair_of == lax.broadcasted_iota(jnp.int32, (own_pairs, wide), 0), 1.0, 0.0
    ).astype(jnp.bfloat16)
    lane_numbers = lax.broadcasted_iota(jnp.int32, (LANES, LANES), 1).astype(jnp.float32)

    def hot_group(group, carry):
        for inner in range(GROUP):
            index = group * GROUP + inner
            lane = (picks[pairs_of(index), :] & (LANES - 1)).astype(jnp.float32)
            wide_lane = jnp.dot(
                lane.T.astype(jnp.bfloat16), select, preferred_element_type=jnp.float32
            )
            for pair in range(own_pairs):
                column = wide_lane[:, pair * LANES : (pair + 1) * LANES]
                column_hots[index, pair] = jnp.where(
                    column == lane_numbers, 1.0, 0.0
                ).astype(jnp.bfloat16)
        return carry

    lax.fori_loop(0, ep_size // GROUP, hot_group, 0)

    @pl.when(my_ep != my_z)
    def _():
        gate_copy(1).wait_recv()

    products = partial[my_z]
    for step in range(1, z_size):
        part_copy(step, my_z).wait_recv()
        products = products + landed[step - 1]
    activated = 0.5 * products * (1.0 + lax.erf(products * (0.5**0.5)))
    weights[my_z] = (gates[...] * activated).astype(jnp.bfloat16)

    def weight_copy(step, owner):
        slot = weights.at[owner]
        return remote(
            slot,
            slot,
            weight_send.at[step - 1],
            weight_recv.at[step - 1],
            my_ep,
            z_at(step) * CORES + my_core,
        )

    for step in range(1, z_size):
        weight_copy(step, my_z).start()

    table_copies[1].wait()
    table_landed(1).wait_recv()

    def near_offset(place):
        half = (place + 1) // 2
        return jnp.where(place % 2 == 1, half, lax.rem(z_size - half, z_size))

    block_ids = lax.broadcasted_iota(jnp.int32, (blocks, LANES), 0)
    block_first = lax.broadcasted_iota(jnp.int32, (blocks, LANES), 1) < per_token

    def out_copy(step, target, cross):
        target_core = other_core if cross else my_core
        return remote(
            summed.at[target_core, target],
            out_landed.at[cross, step],
            out_send.at[cross, step],
            out_recv.at[cross, step],
            target,
            my_z * CORES + target_core,
        )

    quarter = fold_rows * CHUNK
    pitch = folds * quarter + PITCH_PAD

    def spread_group(first, place):
        offsets = [near_offset(first + place + inner) for inner in range(GROUP)]
        for offset in offsets:

            @pl.when(offset != 0)
            def _():
                weight_copy(z_size - offset, z_at(offset)).wait_recv()

        for inner in range(GROUP):
            index = z_at(offsets[inner])
            slice_weights = weights[index].astype(jnp.float32)
            for pair in range(own_pairs):
                row = picks[pl.ds(index * own_pairs + pair, 1), :] - first_row
                block_mask = lax.shift_right_arithmetic(row, 7) == block_ids
                hot = jnp.where(block_mask, slice_weights[pair : pair + 1], 0.0)
                both = jnp.concatenate(
                    [
                        jnp.where(block_first, hot, 0.0).astype(jnp.bfloat16),
                        jnp.where(block_first, 0.0, hot).astype(jnp.bfloat16),
                    ],
                    axis=0,
                )
                placed = jnp.dot(
                    both, column_hots[index, pair], preferred_element_type=jnp.float32
                )
                for half in range(2):
                    fold, row_in_fold = divmod(half * own_pairs + pair, fold_rows)
                    target = fold * quarter + (place + inner) * fold_rows + row_in_fold
                    spread[pl.ds(target, blocks, stride=pitch), :] = placed[
                        half * blocks : (half + 1) * blocks
                    ]

    def spread_chunk(first):
        rows = jnp.concatenate(
            [
                spread[block * pitch : block * pitch + folds * quarter, :].astype(
                    jnp.bfloat16
                )
                for block in range(blocks)
            ],
            axis=1,
        )
        total = matmul_nt(rows, value[...])
        targets = [z_at(near_offset(first + inner)) for inner in range(CHUNK)]
        for core in range(CORES):
            piece = jnp.concatenate(
                [
                    total[
                        fold * quarter : (fold + 1) * quarter,
                        core * width : (core + 1) * width,
                    ]
                    for fold in range(folds)
                ],
                axis=1,
            )
            for inner in range(CHUNK):
                summed[core, targets[inner]] = piece[
                    inner * fold_rows : (inner + 1) * fold_rows
                ]
        for inner in range(CHUNK):
            target = targets[inner]
            step = ep_step(target)

            @pl.when(step != 0)
            def _():
                out_copy(step, target, 0).start()

            out_copy(step, target, 1).start()

    def spread_step(chunk, carry):
        def step(group, inner_carry):
            spread_group(chunk * CHUNK, group * GROUP)
            return inner_carry

        lax.fori_loop(0, CHUNK // GROUP, step, 0)
        spread_chunk(chunk * CHUNK)
        return carry

    lax.fori_loop(0, z_size // CHUNK, spread_step, 0)

    result = summed[my_core, my_ep]
    for cross in range(CORES):
        for step in range(1 - cross, ep_size):
            out_copy(step, my_ep, cross).wait_recv()
            result = result + out_landed[cross, step]
    out_ref[...] = unfolded(result).astype(out_ref.dtype)

    for step in range(1, ep_size):
        feature_copy(step, my_ep, my_core, 0).wait_send()
        feature_copy(step, my_ep, my_core, 1).wait_send()
        pick_copy(step, my_ep).wait_send()
    feature_copy(0, my_ep, my_core, 1).wait_send()

    @pl.when(my_ep == my_z)
    def _():
        for step in range(1, ep_size):
            gate_copy(step).wait_send()

    for number in range(2):
        table_copy(number).wait_send()
    for step in range(1, z_size):
        part_copy(step, z_at(step)).wait_send()
        weight_copy(step, my_z).wait_send()
    for cross in range(CORES):
        for step in range(1 - cross, ep_size):
            out_copy(step, ep_at(step), cross).wait_send()


def shards(ep_size, tp_size, features, key_table, value_table, chosen, scores):
    own_tokens, width = features.shape
    _, heads, top = chosen.shape
    half_rows = key_table.shape[0] // CORES
    z_size = tp_size // CORES
    tokens = ep_size * own_tokens
    own_pairs = own_tokens // 2
    blocks = half_rows // LANES
    chunk_tokens = CHUNK * own_tokens
    dma = pltpu.SemaphoreType.DMA
    slices = (z_size, own_pairs, LANES)
    folded = (own_tokens * width // LANES, LANES)
    return pl.pallas_call(
        functools.partial(kernel, ep_size, z_size),
        out_shape=pltpu.VMEM((own_tokens, width), jnp.bfloat16),
        in_specs=[pl.BlockSpec(memory_space=pl.ANY)] * 5,
        out_specs=pl.BlockSpec(memory_space=pltpu.VMEM),
        scratch_shapes=[
            pltpu.VMEM((own_tokens, width), features.dtype),
            pltpu.VMEM((CORES, ep_size) + folded, features.dtype),
            pltpu.VMEM((tokens, CORES * width), features.dtype),
            pltpu.VMEM((own_tokens, heads, top), jnp.int32),
            pltpu.VMEM((own_tokens, heads, top), jnp.float32),
            pltpu.VMEM((tokens // 2, LANES), jnp.int32),
            pltpu.VMEM((own_pairs, LANES), jnp.float32),
            pltpu.VMEM((CORES * width, half_rows), key_table.dtype),
            pltpu.VMEM((CORES * width, half_rows), value_table.dtype),
            pltpu.VMEM((GROUP * own_tokens, UNROLL * LANES), jnp.float32),
            pltpu.VMEM((GROUP * own_tokens, UNROLL * LANES), jnp.float32),
            pltpu.VMEM(slices, jnp.float32),
            pltpu.VMEM((z_size - 1,) + slices[1:], jnp.float32),
            pltpu.VMEM(slices, jnp.bfloat16),
            pltpu.VMEM((ep_size, own_pairs, LANES, LANES), jnp.bfloat16),
            pltpu.VMEM((blocks * (chunk_tokens + PITCH_PAD), LANES), jnp.float32),
            pltpu.VMEM((CORES, ep_size) + folded, jnp.float32),
            pltpu.VMEM((CORES, ep_size) + folded, jnp.float32),
            pltpu.SemaphoreType.REGULAR,
            dma((5,)),
            dma((2,)),
            dma((2,)),
            dma((CORES, ep_size)),
            dma((CORES, ep_size)),
            dma((ep_size - 1,)),
            dma((ep_size - 1,)),
            dma((ep_size - 1,)),
            dma((1,)),
            dma((z_size - 1,)),
            dma((z_size - 1,)),
            dma((z_size - 1,)),
            dma((z_size - 1,)),
            dma((CORES, ep_size)),
            dma((CORES, ep_size)),
        ],
        compiler_params=pltpu.CompilerParams(collective_id=0, has_side_effects=True),
    )(features, key_table.T, value_table.T, chosen, scores)


def solution(mesh):
    return jax.shard_map(
        functools.partial(shards, mesh.shape["ep"], mesh.shape["tp"]),
        mesh=mesh,
        in_specs=(
            P("ep", "tp"),
            P("ep", "tp"),
            P("ep", "tp"),
            P("ep", None, None),
            P("ep", None, None),
        ),
        out_specs=P("ep", "tp"),
        check_vma=False,
    )
```
